512 devices in a mesh: grp: 2 (over y), row: 32 (over z, core), col: 8 (over x).
Axes of the slice: x: 8, y: 2, z: 16, core: 2. Of those that a mesh axis runs over, the one named last changes fastest.
The devices are a block of a 8x8x16 slice.
Arguments:
- gate_one: bfloat16 [16384, 2048], P(('grp', 'row'), 'col'), parts along dimension 0, may hold values from -6 to 6
- gate_two: bfloat16 [16384, 2048], P(('grp', 'row'), 'col'), parts along dimension 0, may hold values from -6 to 6
- values: bfloat16 [16384, 2048], P(('grp', 'row'), 'col'), parts along dimension 0, may hold values from -6 to 6
- conv_taps: bfloat16 [3, 3, 2048], P(None, None, 'col'), may hold values from -3 to 3
- embed_weight: float32 [33, 128], replicated, may hold values from -12 to 12
- embed_bias: float32 [128], replicated, may hold values from -3.140625 to 3.140625
- sine_freq: float32 [128], replicated, may hold values from 0.1 to 1.9
- inner_weight: float32 [128, 128], replicated, may hold values from -6 to 6
- inner_bias: float32 [128], replicated, may hold values from -3.140625 to 3.140625
- filter_weight: float32 [128, 2, 2, 2048], P(None, None, None, 'col'), may hold values from -0.5 to 0.5
- decay_rate: float32 [2, 2, 2048], P(None, None, 'col'), may hold values from 0.3 to 655.36
- skip_gain: float32 [2, 2048], P(None, 'col'), may hold values from -4 to 4
- out_weight: bfloat16 [2048, 4096], P(None, 'col'), may hold values from -0.125 to 0.125
Outputs:
- mixed: bfloat16 [16384, 4096], P(('grp', 'row'), 'col'), parts along dimension 0
The draws below stay inside these ranges and needn't reach their ends.
There are 2 independent parts, one for each index of `grp`. The reference program is written for one: setup_inputs(seed, part) draws one part's arguments, and reference() takes and returns one part's arrays. A program takes and returns all parts, laid end to end along the dimension named above; an argument that names none is the same for every part. Nothing has to cross between parts.
All inputs are finite; a program needn't handle non-finite values.
Results may differ from the reference program's by a relative error of at most 0.015.
Values may be sent and summed in bfloat16 or wider, within the bound.
No kernel may reach another device: no remote copies, remote signals or barrier semaphores. Data moves between devices by JAX's collectives and lax.ppermute only.
A program may use at most 64 MiB of HBM per device.

```python
import math
import jax
import jax.numpy as jnp
from jax import lax

D = 4096
WIDTH = 2048
FILTER_HIDDEN = 128
EMBED = 33
ORDERS = 2
SEQ = 8192


def draw_decay_rate(key, part):
    rate_shape = (ORDERS, 2, WIDTH)
    pick_key, slow_key, fast_key = jax.random.split(key, 3)
    slow_rate = jax.random.uniform(slow_key, rate_shape, jnp.float32, 0.3, 2.3)
    low_log = jnp.log(jnp.float32(0.02 * SEQ))
    high_log = jnp.log(jnp.float32(0.08 * SEQ))
    fast_rate = jnp.exp(jax.random.uniform(fast_key, rate_shape, jnp.float32, low_log, high_log))
    fast_share = 0.5
    is_fast = jax.random.uniform(pick_key, rate_shape, jnp.float32) < fast_share
    return jnp.where(is_fast, fast_rate, slow_rate)


def shard_levels(rng, dims, pieces, least, largest):
    def one(dim, parts):
        steps = jax.random.uniform(jax.random.fold_in(jax.random.fold_in(rng, 6), dim), (parts,), jnp.float32, least / len(pieces), largest / len(pieces))
        return jnp.repeat(jnp.exp(steps), dims[dim] // parts).reshape((-1,) + (1,) * (len(dims) - dim - 1))

    loudness = one(*pieces[0])
    for cut in pieces[1:]:
        loudness = loudness * one(*cut)
    return loudness


def scatter_about(key, extent, deviation, bound, cuts=(), kind=jnp.bfloat16):
    array = jax.random.normal(key, extent, jnp.float32) * deviation
    if len(cuts) > 0:
        array = shard_levels(key, extent, cuts, -0.22, 0.18) * array
    return jnp.clip(array, min=-bound, max=bound).astype(kind)


def setup_inputs(seed: int = 0, part: int = 0) -> dict:
    seeds = jax.random.split(jax.random.key(seed), 14)
    own_keys = jax.random.split(jax.random.fold_in(seeds[13], part), 14)
    return {
        "gate_one": scatter_about(own_keys[0], (SEQ, WIDTH), 1.0, 6.0, ((0, 32), (1, 8))),
        "gate_two": scatter_about(own_keys[1], (SEQ, WIDTH), 1.0, 6.0, ((0, 32), (1, 8))),
        "values": scatter_about(own_keys[2], (SEQ, WIDTH), 1.0, 6.0, ((0, 32), (1, 8))),
        "conv_taps": scatter_about(seeds[3], (3, 3, WIDTH), 0.577, 3.0, ((2, 8),)),
        "embed_weight": scatter_about(seeds[4], (EMBED, FILTER_HIDDEN), 3.0, 12.0, (), jnp.float32),
        "embed_bias": jnp.clip(jax.random.uniform(seeds[5], (FILTER_HIDDEN,), jnp.float32, -3.140625, 3.140625), -3.140625, 3.140625),
        "sine_freq": jnp.clip(1.0 + 0.18 * jax.random.normal(seeds[6], (FILTER_HIDDEN,), jnp.float32), 0.1, 1.9),
        "inner_weight": scatter_about(seeds[7], (FILTER_HIDDEN, FILTER_HIDDEN), 1.5, 6.0, (), jnp.float32),
        "inner_bias": jnp.clip(jax.random.uniform(seeds[8], (FILTER_HIDDEN,), jnp.float32, -3.140625, 3.140625), -3.140625, 3.140625),
        "filter_weight": scatter_about(seeds[9], (FILTER_HIDDEN, ORDERS, 2, WIDTH), FILTER_HIDDEN ** -0.5, 0.5, ((3, 8),), jnp.float32),
        "decay_rate": draw_decay_rate(jax.random.fold_in(seeds[13], 71), part),
        "skip_gain": scatter_about(seeds[11], (ORDERS, WIDTH), 1.0, 4.0, ((1, 8),), jnp.float32),
        "out_weight": scatter_about(seeds[12], (WIDTH, D), WIDTH ** -0.5, 0.125, ((1, 8),)),
    }


HIGHEST = lax.Precision.HIGHEST
ENERGY_FLOOR = 1.0

def filter_hidden(lag_vals, seq_len, embed_weight, embed_bias, sine_freq, inner_weight, inner_bias):
    band_count = (embed_weight.shape[0] - 1) // 2
    lag_float = lag_vals.astype(jnp.float32)
    band_list = jnp.linspace(0.0001, band_count - 1, band_count, dtype=jnp.float32)
    phases = 2.0 * math.pi / seq_len * lag_float[:, None] * band_list[None, :]
    features = jnp.concatenate([(lag_float / seq_len)[:, None], jnp.cos(phases), -jnp.sin(phases)], axis=1)
    layer_one = jnp.sin(sine_freq * (jnp.dot(features, embed_weight, precision=HIGHEST) + embed_bias))
    return jnp.sin(sine_freq * (jnp.dot(layer_one, inner_weight, precision=HIGHEST) + inner_bias))

def reference(gate_one, gate_two, values, conv_taps, embed_weight, embed_bias, sine_freq, inner_weight, inner_bias, filter_weight, decay_rate, skip_gain, out_weight):
    seq_len = gate_one.shape[0]
    stacked = jnp.stack([gate_one, gate_two, values]).astype(jnp.float32)
    padded = jnp.pad(stacked, ((0, 0), (1, 1), (0, 0)))
    tap_vals = conv_taps.astype(jnp.float32)
    short_conv = padded[:, :-2] * tap_vals[:, 0][:, None] + padded[:, 1:-1] * tap_vals[:, 1][:, None] + padded[:, 2:] * tap_vals[:, 2][:, None]
    lag_vals = jnp.arange(seq_len, dtype=jnp.int32)
    hidden = filter_hidden(lag_vals, seq_len, embed_weight, embed_bias, sine_freq, inner_weight, inner_bias)
    raw_taps = jnp.einsum('mh,hodc->modc', hidden, filter_weight, precision=HIGHEST, preferred_element_type=jnp.float32)
    ratio = lag_vals.astype(jnp.float32) / seq_len
    raw_taps = raw_taps * jnp.exp(-ratio[:, None, None, None] * decay_rate[None])
    forward_taps = raw_taps[:, :, 0]
    backward_taps = raw_taps[:, :, 1]
    all_taps = jnp.concatenate([forward_taps, jnp.zeros_like(forward_taps[:1]), jnp.flip(backward_taps[1:], axis=0)], axis=0)
    all_taps = all_taps * lax.rsqrt(lax.optimization_barrier(jnp.sum(all_taps * all_taps, axis=0, keepdims=True)) + ENERGY_FLOOR)
    spectrum = jnp.fft.rfft(all_taps, axis=0)
    current = short_conv[2]
    for order_idx in range(skip_gain.shape[0]):
        wave_data = jnp.fft.rfft(current, n=2 * seq_len, axis=0)
        long_part = jnp.fft.irfft(wave_data * spectrum[:, order_idx], n=2 * seq_len, axis=0)[:seq_len]
        current = short_conv[order_idx] * (long_part + skip_gain[order_idx] * current)
    gated_out = current.astype(jnp.bfloat16)
    return jnp.dot(gated_out, out_weight, preferred_element_type=jnp.float32).astype(jnp.bfloat16)
```

```python
import functools
import math

import jax
import jax.numpy as jnp
import numpy as np
from jax import lax
from jax.experimental import pallas as pl
from jax.experimental.pallas import tpu as pltpu
from jax.sharding import PartitionSpec as P

ENERGY_FLOOR = 1.0
F32 = jnp.float32
BF16 = jnp.bfloat16


def halves(value):
    high = value.astype(BF16)
    return high, (value - high.astype(F32)).astype(BF16)


def thirds(value):
    high = value.astype(BF16)
    rest = value - high.astype(F32)
    middle = rest.astype(BF16)
    return high, middle, (rest - middle.astype(F32)).astype(BF16)


def dot(left, right):
    return jnp.dot(left, right, preferred_element_type=F32)


def dot_three(left_high, left_low, right_high, right_low):
    return dot(left_high, right_high) + dot(left_low, right_high) + dot(left_high, right_low)


def cos_turns(turns):
    near = turns - jnp.round(turns)
    quarter = jnp.abs(near) - 0.25
    square = quarter * quarter
    total = jnp.full_like(square, SINE[-1])
    for factor in SINE[-2::-1]:
        total = total * square + factor
    return total * quarter


def fit_sine():
    nodes = 0.25 * np.cos(np.pi * (np.arange(64) + 0.5) / 128)
    powers = np.stack([nodes ** (2 * i + 1) for i in range(6)], 1)
    return [float(v) for v in np.linalg.lstsq(powers, -np.sin(2 * np.pi * nodes), rcond=None)[0]]


SINE = fit_sine()


def split_constant(table):
    high = table.astype(np.float32).astype(jnp.bfloat16)
    return np.stack([high, (table - high.astype(np.float64)).astype(np.float32).astype(jnp.bfloat16)])


@functools.lru_cache
def tables(rows, chan, block):
    waves = 2 * rows
    half = np.arange(rows + 1)
    phase = 2 * np.pi * (half[:, None] * np.arange(rows)[None] % waves) / waves
    weight = np.where((half == 0) | (half == rows), 1.0, 2.0)[:, None] / (waves * block)
    eye = np.eye(chan)
    into = np.concatenate([np.kron(np.cos(phase), eye), np.kron(-np.sin(phase[1:-1]), eye)])
    back = np.concatenate(
        [np.kron(weight * np.cos(phase), eye), np.kron(-(weight * np.sin(phase))[1:-1], eye)]
    ).T
    inner = 2 * np.pi * (np.arange(block)[:, None] * np.arange(block)[None] % block) / block
    fourier = np.concatenate([np.cos(inner), np.sin(inner)], 1)
    turn = 2 * np.pi * half[:, None] * np.arange(block)[None] / (waves * block)
    twiddle = np.stack([np.cos(turn), np.sin(turn)]).astype(np.float32)
    return split_constant(into), split_constant(back), split_constant(fourier), twiddle


def spread(twiddle_ref, part, chan):
    value = twiddle_ref[part]
    return jnp.broadcast_to(value[:, None, :], (value.shape[0], chan, value.shape[1])).reshape(-1, value.shape[1])


def forward(field, into_ref, fourier_ref, twiddle_ref, chan):
    block = field.shape[1]
    edge = field.shape[0] + chan
    high, low = halves(field)
    mixed = dot_three(into_ref[0], into_ref[1], high, low)
    zero = jnp.zeros((chan, block), F32)
    part_re = mixed[:edge]
    part_im = jnp.concatenate([zero, mixed[edge:], zero], 0)
    cos_part, sin_part = spread(twiddle_ref, 0, chan), spread(twiddle_ref, 1, chan)
    turned = jnp.concatenate(
        [part_re * cos_part + part_im * sin_part, part_im * cos_part - part_re * sin_part], 0
    )
    high, low = halves(turned)
    wave = dot_three(high, low, fourier_ref[0], fourier_ref[1])
    return wave[:edge, :block] + wave[edge:, block:], wave[edge:, :block] - wave[:edge, block:]


def backward(part_re, part_im, back_ref, fourier_ref, twiddle_ref, chan):
    edge, block = part_re.shape
    high, low = halves(jnp.concatenate([part_re, part_im], 0))
    wave = dot_three(high, low, fourier_ref[0], fourier_ref[1])
    part_re = wave[:edge, :block] - wave[edge:, block:]
    part_im = wave[:edge, block:] + wave[edge:, :block]
    cos_part, sin_part = spread(twiddle_ref, 0, chan), spread(twiddle_ref, 1, chan)
    turned_re = part_re * cos_part - part_im * sin_part
    turned_im = part_re * sin_part + part_im * cos_part
    high, low = halves(jnp.concatenate([turned_re, turned_im[chan : edge - chan]], 0))
    return dot_three(back_ref[0], back_ref[1], high, low)


def filter_kernel(
    rows, chan, embed_ref, first_bias_ref, freq_ref, inner_ref, second_bias_ref, weight_ref, decay_ref,
    band_ref, into_ref, fourier_ref, twiddle_ref, spec_re_ref, spec_im_ref,
    first_table, second_table, taps_ref, energy_ref, near_ref, far_ref, first_w, second_w, last_w,
):
    block = taps_ref.shape[2]
    hidden = freq_ref.shape[1]
    seq_len = rows * block
    freq = freq_ref[...] * (0.5 / math.pi)
    w_one, w_two, w_three = thirds(embed_ref[...] * freq)
    none = jnp.zeros_like(w_one)
    first_w[:, :hidden] = jnp.concatenate([w_one, w_one, w_one, w_three], 0)
    first_w[:, hidden:] = jnp.concatenate([w_two, w_two, none, none], 0)
    v_one, v_two = halves(inner_ref[...] * freq)
    second_w[:, :hidden] = jnp.concatenate([v_one, v_one], 0)
    second_w[:, hidden:] = jnp.concatenate([v_two, v_two], 0)
    u_one, u_two = halves(weight_ref[...])
    last_w[:, :hidden] = jnp.concatenate([u_one, u_two], 0)
    last_w[:, hidden:] = jnp.concatenate([u_one, jnp.zeros_like(u_two)], 0)
    first_bias = first_bias_ref[...] * freq - 0.25
    second_bias = second_bias_ref[...] * freq - 0.25
    band = band_ref[0:1]
    shift = band_ref[1:2]
    line = band_ref[2:3]
    lag = lax.broadcasted_iota(jnp.int32, (block, 2 * embed_ref.shape[0]), 0).astype(F32)
    turns = lag * band * (1.0 / seq_len)
    first_table[...] = jnp.where(line > 0, 1.0, cos_turns(turns + shift))
    second_table[...] = jnp.where(line > 0, lag * (1.0 / seq_len), cos_turns(turns + (shift + 0.25)))
    start = lax.broadcasted_iota(jnp.int32, (rows, 2 * embed_ref.shape[0]), 0).astype(F32)
    turns = start * band * (1.0 / rows)
    near_ref[...] = jnp.where(line > 0, start * (1.0 / rows), cos_turns(turns))
    far_ref[...] = jnp.where(line > 0, 1.0, cos_turns(turns - 0.25))
    energy_ref[...] = jnp.zeros_like(energy_ref)
    decay = decay_ref[...]
    lanes = lax.broadcasted_iota(jnp.int32, (1, block), 1)
    left = lax.broadcasted_iota(jnp.int32, (1, 2 * embed_ref.shape[0]), 1) < embed_ref.shape[0]
    parts = weight_ref.shape[0]
    is_back = (lax.broadcasted_iota(jnp.int32, (parts, 1), 0) // chan) % 2 == 1

    @pl.loop(0, rows)
    def _(row):
        feature = first_table[...] * near_ref[pl.ds(row, 1), :] + second_table[...] * far_ref[pl.ds(row, 1), :]
        x_one, x_two, x_three = thirds(feature)
        stacked = jnp.concatenate([jnp.where(left, x_one, x_two), jnp.where(left, x_three, x_one)], 1)
        both = dot(stacked, first_w[...])
        layer_one = cos_turns(both[:, :hidden] + both[:, hidden:] + first_bias)
        y_one, y_two = halves(layer_one)
        both = dot(jnp.concatenate([y_one, y_two], 1), second_w[...])
        layer_two = cos_turns(both[:, :hidden] + both[:, hidden:] + second_bias)
        z_one, z_two = halves(layer_two)
        both = lax.dot_general(
            last_w[...], jnp.concatenate([z_one, z_two], 1), (((1,), (1,)), ((), ())), preferred_element_type=F32
        )
        raw = both[:parts] + both[parts:]
        at = lanes + row * block
        taps = raw * jnp.exp(decay * (at.astype(F32) * (-1.0 / seq_len)))
        taps = jnp.where(is_back & (at == 0), 0.0, taps)
        energy_ref[...] += taps * taps
        place = pl.multiple_of(row * chan, chan)
        for k in range(parts // chan):
            taps_ref[k, pl.ds(place, chan), :] = taps[k * chan : (k + 1) * chan]

    total = jnp.sum(energy_ref[...], axis=1, keepdims=True)

    for order in range(parts // (2 * chan)):
        base = order * 2 * chan
        scale = lax.rsqrt(total[base : base + chan] + total[base + chan : base + 2 * chan] + ENERGY_FLOOR)
        scale = jnp.broadcast_to(scale[None], (rows + 1, chan, block)).reshape(-1, block)
        ahead_re, ahead_im = forward(taps_ref[2 * order], into_ref, fourier_ref, twiddle_ref, chan)
        behind_re, behind_im = forward(taps_ref[2 * order + 1], into_ref, fourier_ref, twiddle_ref, chan)
        spec_re_ref[order] = (ahead_re + behind_re) * scale
        spec_im_ref[order] = (ahead_im - behind_im) * scale


def short(signal, taps, first, rows, chan):
    block = signal.shape[1]
    lanes = lax.broadcasted_iota(jnp.int32, signal.shape, 1)
    line = lax.broadcasted_iota(jnp.int32, signal.shape, 0)
    size = signal.shape[0]
    before = pltpu.roll(signal, 1, 1)
    crossed = jnp.where(line < chan, 0.0, pltpu.roll(before, chan, 0))
    before = jnp.where(lanes == 0, crossed, before)
    after = pltpu.roll(signal, block - 1, 1)
    crossed = jnp.where(line >= size - chan, 0.0, pltpu.roll(after, size - chan, 0))
    after = jnp.where(lanes == block - 1, crossed, after)

    def tap(k):
        column = taps[:, first + k : first + k + 1]
        return jnp.broadcast_to(column[None], (rows, chan, block)).reshape(size, block)

    return before * tap(0) + signal * tap(1) + after * tap(2)


def conv_kernel(
    rows, chan, orders, arrived_ref, param_ref, spec_re_ref, spec_im_ref, into_ref, back_ref, fourier_ref,
    twiddle_ref, out_ref,
):
    block = arrived_ref.shape[2]
    size = rows * chan
    param = param_ref[...]

    def signal(k):
        return arrived_ref[:, k * chan : (k + 1) * chan, :].astype(F32).reshape(size, block)

    current = short(signal(0), param, 6, rows, chan)
    for order in range(orders):
        data_re, data_im = forward(current, into_ref, fourier_ref, twiddle_ref, chan)
        spec_re, spec_im = spec_re_ref[order], spec_im_ref[order]
        long_part = backward(
            data_re * spec_re - data_im * spec_im,
            data_re * spec_im + data_im * spec_re,
            back_ref, fourier_ref, twiddle_ref, chan,
        )
        column = param[:, 9 + order : 10 + order]
        skip = jnp.broadcast_to(column[None], (rows, chan, block)).reshape(size, block)
        current = long_part + skip * current
        if order < orders - 1:
            current = current * short(signal(order + 1), param, 3 * order, rows, chan)
    out_ref[...] = current.astype(BF16).reshape(rows, chan, block)


def turn_kernel(first_ref, second_ref, out_ref):
    rows = out_ref.shape[0]
    chan = out_ref.shape[1] // 2
    for k, ref in enumerate((first_ref, second_ref)):
        turned = jnp.transpose(ref[...].astype(F32)).astype(BF16)
        out_ref[:, k * chan : (k + 1) * chan, :] = turned.reshape(rows, chan, -1)


def gate_kernel(mixed_ref, gate_ref, halo_ref, taps_ref, out_ref):
    gate = gate_ref[...].astype(F32)
    block = gate.shape[0]
    line = lax.broadcasted_iota(jnp.int32, gate.shape, 0)
    halo = halo_ref[...].astype(F32)
    taps = taps_ref[...].astype(F32)
    before = jnp.where(line == 0, halo[0:1], pltpu.roll(gate, 1, 0))
    after = jnp.where(line == block - 1, halo[1:2], pltpu.roll(gate, block - 1, 0))
    factor = before * taps[0:1] + gate * taps[1:2] + after * taps[2:3]
    out_ref[...] = (jnp.transpose(mixed_ref[...].astype(F32)) * factor).astype(BF16)


def call(kernel, out_shape, scratch=(), flops=0, moved=0):
    return pl.pallas_call(
        kernel,
        out_shape=out_shape,
        scratch_shapes=scratch,
        cost_estimate=pl.CostEstimate(flops=flops, bytes_accessed=moved, transcendentals=0),
    )


def per_device(
    gate_one, gate_two, values, conv_taps, embed_weight, embed_bias, sine_freq, inner_weight, inner_bias,
    filter_weight, decay_rate, skip_gain, out_weight,
):
    rows = lax.axis_size("row")
    own = lax.axis_index("row")
    block, columns = gate_one.shape
    orders = skip_gain.shape[0]
    chan = columns // rows
    offset = own * chan
    hidden = sine_freq.shape[0]
    features = embed_weight.shape[0]
    bands = (features - 1) // 2
    into, back, fourier, twiddle = tables(rows, chan, block)

    turned = call(turn_kernel, jax.ShapeDtypeStruct((rows, 2 * chan, block), BF16))(values, gate_one)
    arrived = lax.all_to_all(turned, "row", 0, 0, tiled=True)

    down = [(k, k + 1) for k in range(rows - 1)]
    up = [(k + 1, k) for k in range(rows - 1)]
    halo = jnp.concatenate(
        [lax.ppermute(gate_two[-1:], "row", down), lax.ppermute(gate_two[:1], "row", up)], 0
    )

    weight_here = lax.dynamic_slice_in_dim(filter_weight, offset, chan, 3)
    weight_here = jnp.transpose(weight_here.reshape(hidden, -1))
    decay_here = lax.dynamic_slice_in_dim(decay_rate, offset, chan, 2).reshape(-1, 1)
    taps_here = lax.dynamic_slice_in_dim(conv_taps, offset, chan, 2).astype(F32).reshape(-1, chan)
    skip_here = lax.dynamic_slice_in_dim(skip_gain, offset, chan, 1)
    param = jnp.transpose(jnp.concatenate([taps_here, skip_here], 0))

    width = 64
    embed = jnp.pad(embed_weight, ((0, width - features), (0, 0)))
    steps = np.linspace(0.0001, bands - 1, bands).astype(np.float32)
    band = np.zeros((3, width), np.float32)
    band[0, 1:features] = np.concatenate([steps, steps])
    band[1, 1 + bands : features] = 0.25
    band[2, 0] = 1
    band[:, features:] = 0
    band = np.concatenate([band, band], 1)

    edge = (rows + 1) * chan
    parts = weight_here.shape[0]
    spec_shape = jax.ShapeDtypeStruct((orders, edge, block), F32)
    spec_re, spec_im = call(
        functools.partial(filter_kernel, rows, chan),
        (spec_shape, spec_shape),
        (
            pltpu.VMEM((block, 2 * width), F32),
            pltpu.VMEM((block, 2 * width), F32),
            pltpu.VMEM((parts // chan, rows * chan, block), F32),
            pltpu.VMEM((parts, block), F32),
            pltpu.VMEM((rows, 2 * width), F32),
            pltpu.VMEM((rows, 2 * width), F32),
            pltpu.VMEM((4 * width, 2 * hidden), BF16),
            pltpu.VMEM((2 * hidden, 2 * hidden), BF16),
            pltpu.VMEM((2 * parts, 2 * hidden), BF16),
        ),
        flops=12_000_000_000,
    )(
        embed, embed_bias[None], sine_freq[None], inner_weight, inner_bias[None], weight_here, decay_here,
        band, into, fourier, twiddle,
    )
    mixed = call(
        functools.partial(conv_kernel, rows, chan, orders),
        jax.ShapeDtypeStruct((rows, chan, block), BF16),
        flops=5_000_000_000,
    )(arrived, param, spec_re, spec_im, into, back, fourier, twiddle)
    mixed = lax.all_to_all(mixed, "row", 0, 0, tiled=True).reshape(columns, block)
    gated = call(gate_kernel, jax.ShapeDtypeStruct((block, columns), BF16))(mixed, gate_two, halo, conv_taps[1])
    return finish(gated, out_weight)


def finish(gated, out_weight):
    peers = lax.axis_size("col")
    block, columns = gated.shape
    half = block // 2
    upper = lax.all_gather(gated[:half], "col", axis=0)
    lower = lax.all_gather(gated[half:], "col", axis=0)
    weight = out_weight.reshape(peers, columns, -1)
    return jnp.concatenate(
        [
            jnp.einsum("crk,ckn->rn", part, weight, preferred_element_type=F32).astype(BF16)
            for part in (upper, lower)
        ],
        0,
    )


def solution(mesh):
    spread_rows = ("grp", "row")
    in_specs = (
        P(spread_rows, "col"),
        P(spread_rows, "col"),
        P(spread_rows, "col"),
        P(None, None, "col"),
        P(),
        P(),
        P(),
        P(),
        P(),
        P(None, None, None, "col"),
        P(None, None, "col"),
        P(None, "col"),
        P(None, "col"),
    )
    return jax.shard_map(
        per_device, mesh=mesh, in_specs=in_specs, out_specs=P(spread_rows, "col"), check_vma=False
    )
```

```python
import functools
import math

import jax
import jax.numpy as jnp
import numpy as np
from jax import lax
from jax.experimental import pallas as pl
from jax.experimental.pallas import tpu as pltpu
from jax.sharding import PartitionSpec as P

ENERGY_FLOOR = 1.0
F32 = jnp.float32
BF16 = jnp.bfloat16


def halves(value):
    high = value.astype(BF16)
    return high, (value - high.astype(F32)).astype(BF16)


def dot(left, right):
    return jnp.dot(left, right, preferred_element_type=F32)


def dot_wide(left_high, left_low, right_high, right_low):
    return dot(
        jnp.concatenate([left_high, left_low, left_high], 1),
        jnp.concatenate([right_high, right_high, right_low], 0),
    )


def cos_turns(turns):
    near = turns - jnp.round(turns)
    quarter = jnp.abs(near) - 0.25
    square = quarter * quarter
    total = jnp.full_like(square, SINE[-1])
    for factor in SINE[-2::-1]:
        total = total * square + factor
    return total * quarter


def fit_sine():
    nodes = 0.25 * np.cos(np.pi * (np.arange(64) + 0.5) / 128)
    powers = np.stack([nodes ** (2 * i + 1) for i in range(5)], 1)
    return [float(v) for v in np.linalg.lstsq(powers, -np.sin(2 * np.pi * nodes), rcond=None)[0]]


SINE = fit_sine()


def split_constant(table):
    high = table.astype(np.float32).astype(jnp.bfloat16)
    return np.stack([high, (table - high.astype(np.float64)).astype(np.float32).astype(jnp.bfloat16)])


@functools.lru_cache
def tables(rows, chan, block):
    waves = 2 * rows
    half = np.arange(rows + 1)
    phase = 2 * np.pi * (half[:, None] * np.arange(rows)[None] % waves) / waves
    weight = np.where((half == 0) | (half == rows), 1.0, 2.0)[:, None] / (waves * block)
    eye = np.eye(chan)
    into = np.concatenate([np.kron(np.cos(phase), eye), np.kron(-np.sin(phase[1:-1]), eye)])
    back = np.concatenate(
        [np.kron(weight * np.cos(phase), eye), np.kron(-(weight * np.sin(phase))[1:-1], eye)]
    ).T
    inner = 2 * np.pi * (np.arange(block)[:, None] * np.arange(block)[None] % block) / block
    pair = np.concatenate([np.cos(inner), np.sin(inner)], 0)
    turn = 2 * np.pi * half[:, None] * np.arange(block)[None] / (waves * block)
    twiddle = np.stack([np.cos(turn), np.sin(turn)]).astype(np.float32)
    return split_constant(into), split_constant(back), split_constant(pair), twiddle


def spread(twiddle_ref, part, chan):
    value = twiddle_ref[part]
    return jnp.broadcast_to(value[:, None, :], (value.shape[0], chan, value.shape[1])).reshape(-1, value.shape[1])


def first_stage(field, into_ref, chan):
    edge = field.shape[0] + chan
    high, low = halves(field)
    part_re = dot_wide(into_ref[0, :edge], into_ref[1, :edge], high, low)
    part_im = dot_wide(into_ref[0, edge:], into_ref[1, edge:], high, low)
    zero = jnp.zeros((chan, field.shape[1]), F32)
    return part_re, jnp.concatenate([zero, part_im, zero], 0)


def pair_product(first, second, pair_ref):
    first_high, first_low = halves(first)
    second_high, second_low = halves(second)
    return dot_wide(
        jnp.concatenate([first_high, second_high], 1),
        jnp.concatenate([first_low, second_low], 1),
        pair_ref[0],
        pair_ref[1],
    )


def forward(field, into_ref, pair_ref, cos_part, sin_part, chan):
    part_re, part_im = first_stage(field, into_ref, chan)
    turned_re = part_re * cos_part + part_im * sin_part
    turned_im = part_im * cos_part - part_re * sin_part
    return pair_product(turned_re, turned_im, pair_ref), pair_product(turned_im, -turned_re, pair_ref)


def backward(part_re, part_im, back_ref, pair_ref, cos_part, sin_part, chan):
    edge = part_re.shape[0]
    wave_re = pair_product(part_re, -part_im, pair_ref)
    wave_im = pair_product(part_im, part_re, pair_ref)
    turned_re = wave_re * cos_part - wave_im * sin_part
    turned_im = wave_re * sin_part + wave_im * cos_part
    high, low = halves(jnp.concatenate([turned_re, turned_im[chan : edge - chan]], 0))
    middle = back_ref.shape[1] // 2
    return jnp.concatenate(
        [
            dot_wide(back_ref[0, :middle], back_ref[1, :middle], high, low),
            dot_wide(back_ref[0, middle:], back_ref[1, middle:], high, low),
        ],
        0,
    )


def filter_kernel(
    rows, chan, embed_ref, first_bias_ref, freq_ref, inner_ref, second_bias_ref, weight_ref, decay_ref,
    band_ref, into_ref, pair_ref, twiddle_ref, spec_re_ref, spec_im_ref,
    first_table, second_table, taps_ref, energy_ref, near_ref, far_ref, first_w, second_w, last_w,
):
    block = taps_ref.shape[2]
    hidden = freq_ref.shape[1]
    seq_len = rows * block
    freq = freq_ref[...] * (0.5 / math.pi)
    w_one, w_two = halves(embed_ref[...] * freq)
    first_w[:, :hidden] = jnp.concatenate([w_one, w_one], 0)
    first_w[:, hidden:] = jnp.concatenate([w_two, w_two], 0)
    v_one, v_two = halves(inner_ref[...] * freq)
    second_w[:, :hidden] = jnp.concatenate([v_one, v_one], 0)
    second_w[:, hidden:] = jnp.concatenate([v_two, v_two], 0)
    u_one, u_two = halves(weight_ref[...])
    last_w[:, :hidden] = jnp.concatenate([u_one, u_two], 0)
    last_w[:, hidden:] = jnp.concatenate([u_one, jnp.zeros_like(u_two)], 0)
    first_bias = first_bias_ref[...] * freq - 0.25
    second_bias = second_bias_ref[...] * freq - 0.25
    band = band_ref[0:1]
    shift = band_ref[1:2]
    line = band_ref[2:3]
    lag = lax.broadcasted_iota(jnp.int32, (block, 2 * embed_ref.shape[0]), 0).astype(F32)
    turns = lag * band * (1.0 / seq_len)
    first_table[...] = jnp.where(line > 0, 1.0, cos_turns(turns + shift))
    second_table[...] = jnp.where(line > 0, lag * (1.0 / seq_len), cos_turns(turns + (shift + 0.25)))
    start = lax.broadcasted_iota(jnp.int32, (rows, 2 * embed_ref.shape[0]), 0).astype(F32)
    turns = start * band * (1.0 / rows)
    near_ref[...] = jnp.where(line > 0, start * (1.0 / rows), cos_turns(turns))
    far_ref[...] = jnp.where(line > 0, 1.0, cos_turns(turns - 0.25))
    energy_ref[...] = jnp.zeros_like(energy_ref)
    decay = decay_ref[...]
    lanes = lax.broadcasted_iota(jnp.int32, (1, block), 1)
    left = lax.broadcasted_iota(jnp.int32, (1, 2 * embed_ref.shape[0]), 1) < embed_ref.shape[0]
    parts = weight_ref.shape[0]
    is_back = (lax.broadcasted_iota(jnp.int32, (parts, 1), 0) // chan) % 2 == 1

    def lags(row):
        feature = first_table[...] * near_ref[pl.ds(row, 1), :] + second_table[...] * far_ref[pl.ds(row, 1), :]
        x_one, x_two = halves(feature)
        both = dot(jnp.where(left, x_one, x_two), first_w[...])
        layer_one = cos_turns(both[:, :hidden] + both[:, hidden:] + first_bias)
        y_one, y_two = halves(layer_one)
        both = dot(jnp.concatenate([y_one, y_two], 1), second_w[...])
        layer_two = cos_turns(both[:, :hidden] + both[:, hidden:] + second_bias)
        z_one, z_two = halves(layer_two)
        both = lax.dot_general(
            last_w[...], jnp.concatenate([z_one, z_two], 1), (((1,), (1,)), ((), ())), preferred_element_type=F32
        )
        raw = both[:parts] + both[parts:]
        at = lanes + row * block
        taps = raw * jnp.exp(decay * (at.astype(F32) * (-1.0 / seq_len)))
        return jnp.where(is_back & (at == 0), 0.0, taps)

    @pl.loop(0, rows // 2)
    def _(step):
        found = [lags(2 * step + k) for k in range(2)]
        energy_ref[...] += found[0] * found[0] + found[1] * found[1]
        for k in range(2):
            place = pl.multiple_of((2 * step + k) * chan, chan)
            for order in range(parts // (2 * chan)):
                base = order * 2 * chan
                ahead = found[k][base : base + chan]
                behind = found[k][base + chan : base + 2 * chan]
                taps_ref[2 * order, pl.ds(place, chan), :] = ahead + behind
                taps_ref[2 * order + 1, pl.ds(place, chan), :] = ahead - behind

    total = jnp.sum(energy_ref[...], axis=1, keepdims=True)
    cos_part, sin_part = spread(twiddle_ref, 0, chan), spread(twiddle_ref, 1, chan)
    for order in range(parts // (2 * chan)):
        base = order * 2 * chan
        scale = lax.rsqrt(total[base : base + chan] + total[base + chan : base + 2 * chan] + ENERGY_FLOOR)
        scale = jnp.broadcast_to(scale[None], (rows + 1, chan, block)).reshape(-1, block)
        even_re, even_im = first_stage(taps_ref[2 * order], into_ref, chan)
        odd_re, odd_im = first_stage(taps_ref[2 * order + 1], into_ref, chan)
        spec_re_ref[order] = scale * pair_product(
            even_re * cos_part + even_im * sin_part, even_im * cos_part - even_re * sin_part, pair_ref
        )
        spec_im_ref[order] = scale * pair_product(
            odd_im * cos_part - odd_re * sin_part, -(odd_re * cos_part + odd_im * sin_part), pair_ref
        )


def short(signal, taps, first, rows, chan):
    block = signal.shape[1]
    lanes = lax.broadcasted_iota(jnp.int32, signal.shape, 1)
    line = lax.broadcasted_iota(jnp.int32, signal.shape, 0)
    size = signal.shape[0]
    before = pltpu.roll(signal, 1, 1)
    crossed = jnp.where(line < chan, 0.0, pltpu.roll(before, chan, 0))
    before = jnp.where(lanes == 0, crossed, before)
    after = pltpu.roll(signal, block - 1, 1)
    crossed = jnp.where(line >= size - chan, 0.0, pltpu.roll(after, size - chan, 0))
    after = jnp.where(lanes == block - 1, crossed, after)

    def tap(k):
        column = taps[:, first + k : first + k + 1]
        return jnp.broadcast_to(column[None], (rows, chan, block)).reshape(size, block)

    return before * tap(0) + signal * tap(1) + after * tap(2)


def conv_kernel(
    rows, chan, orders, arrived_ref, param_ref, spec_re_ref, spec_im_ref, into_ref, back_ref, pair_ref,
    twiddle_ref, out_ref,
):
    block = arrived_ref.shape[2]
    size = rows * chan
    param = param_ref[...]

    def signal(k):
        return arrived_ref[:, k * chan : (k + 1) * chan, :].astype(F32).reshape(size, block)

    cos_part, sin_part = spread(twiddle_ref, 0, chan), spread(twiddle_ref, 1, chan)
    current = short(signal(0), param, 6, rows, chan)
    for order in range(orders):
        data_re, data_im = forward(current, into_ref, pair_ref, cos_part, sin_part, chan)
        spec_re, spec_im = spec_re_ref[order], spec_im_ref[order]
        long_part = backward(
            data_re * spec_re - data_im * spec_im,
            data_re * spec_im + data_im * spec_re,
            back_ref, pair_ref, cos_part, sin_part, chan,
        )
        column = param[:, 9 + order : 10 + order]
        skip = jnp.broadcast_to(column[None], (rows, chan, block)).reshape(size, block)
        current = long_part + skip * current
        if order < orders - 1:
            current = current * short(signal(order + 1), param, 3 * order, rows, chan)
    out_ref[...] = current.astype(BF16).reshape(rows, chan, block)


def turn_kernel(first_ref, second_ref, out_ref):
    rows = out_ref.shape[0]
    chan = out_ref.shape[1] // 2
    for k, ref in enumerate((first_ref, second_ref)):
        turned = jnp.transpose(ref[...].astype(F32)).astype(BF16)
        out_ref[:, k * chan : (k + 1) * chan, :] = turned.reshape(rows, chan, -1)


def gate_kernel(mixed_ref, gate_ref, halo_ref, taps_ref, out_ref):
    gate = gate_ref[...].astype(F32)
    block = gate.shape[0]
    line = lax.broadcasted_iota(jnp.int32, gate.shape, 0)
    halo = halo_ref[...].astype(F32)
    taps = taps_ref[...].astype(F32)
    before = jnp.where(line == 0, halo[0:1], pltpu.roll(gate, 1, 0))
    after = jnp.where(line == block - 1, halo[1:2], pltpu.roll(gate, block - 1, 0))
    factor = before * taps[0:1] + gate * taps[1:2] + after * taps[2:3]
    gated = (jnp.transpose(mixed_ref[...].astype(F32)) * factor).astype(BF16)
    for peer in range(out_ref.shape[0]):
        out_ref[peer] = gated


def call(kernel, out_shape, scratch=(), flops=0, limit=12):
    return pl.pallas_call(
        kernel,
        out_shape=out_shape,
        scratch_shapes=scratch,
        cost_estimate=pl.CostEstimate(flops=flops, bytes_accessed=0, transcendentals=0),
        compiler_params=pltpu.CompilerParams(vmem_limit_bytes=limit << 20),
    )


def per_device(
    gate_one, gate_two, values, conv_taps, embed_weight, embed_bias, sine_freq, inner_weight, inner_bias,
    filter_weight, decay_rate, skip_gain, out_weight,
):
    rows = lax.axis_size("row")
    own = lax.axis_index("row")
    block, columns = gate_one.shape
    orders = skip_gain.shape[0]
    chan = columns // rows
    offset = own * chan
    hidden = sine_freq.shape[0]
    features = embed_weight.shape[0]
    peers = lax.axis_size("col")
    bands = (features - 1) // 2
    into, back, pair, twiddle = tables(rows, chan, block)

    turned = call(turn_kernel, jax.ShapeDtypeStruct((rows, 2 * chan, block), BF16))(values, gate_one)
    arrived = lax.all_to_all(turned, "row", 0, 0, tiled=True)

    down = [(k, k + 1) for k in range(rows - 1)]
    up = [(k + 1, k) for k in range(rows - 1)]
    halo = jnp.concatenate(
        [lax.ppermute(gate_two[-1:], "row", down), lax.ppermute(gate_two[:1], "row", up)], 0
    )

    weight_here = lax.dynamic_slice_in_dim(filter_weight, offset, chan, 3)
    weight_here = jnp.transpose(weight_here.reshape(hidden, -1))
    decay_here = lax.dynamic_slice_in_dim(decay_rate, offset, chan, 2).reshape(-1, 1)
    taps_here = lax.dynamic_slice_in_dim(conv_taps, offset, chan, 2).astype(F32).reshape(-1, chan)
    skip_here = lax.dynamic_slice_in_dim(skip_gain, offset, chan, 1)
    param = jnp.transpose(jnp.concatenate([taps_here, skip_here], 0))

    width = 64
    embed = jnp.pad(embed_weight, ((0, width - features), (0, 0)))
    steps = np.linspace(0.0001, bands - 1, bands).astype(np.float32)
    band = np.zeros((3, width), np.float32)
    band[0, 1:features] = np.concatenate([steps, steps])
    band[1, 1 + bands : features] = 0.25
    band[2, 0] = 1
    band[:, features:] = 0
    band = np.concatenate([band, band], 1)

    edge = (rows + 1) * chan
    parts = weight_here.shape[0]
    spec_shape = jax.ShapeDtypeStruct((orders, edge, block), F32)
    spec_re, spec_im = call(
        functools.partial(filter_kernel, rows, chan),
        (spec_shape, spec_shape),
        (
            pltpu.VMEM((block, 2 * width), F32),
            pltpu.VMEM((block, 2 * width), F32),
            pltpu.VMEM((parts // chan, rows * chan, block), F32),
            pltpu.VMEM((parts, block), F32),
            pltpu.VMEM((rows, 2 * width), F32),
            pltpu.VMEM((rows, 2 * width), F32),
            pltpu.VMEM((2 * width, 2 * hidden), BF16),
            pltpu.VMEM((2 * hidden, 2 * hidden), BF16),
            pltpu.VMEM((2 * parts, 2 * hidden), BF16),
        ),
        flops=12_000_000_000,
        limit=20,
    )(
        embed, embed_bias[None], sine_freq[None], inner_weight, inner_bias[None], weight_here, decay_here,
        band, into, pair, twiddle,
    )
    mixed = call(
        functools.partial(conv_kernel, rows, chan, orders),
        jax.ShapeDtypeStruct((rows, chan, block), BF16),
        flops=5_000_000_000,
        limit=20,
    )(arrived, param, spec_re, spec_im, into, back, pair, twiddle)
    mixed = lax.all_to_all(mixed, "row", 0, 0, tiled=True).reshape(columns, block)
    gated = call(gate_kernel, jax.ShapeDtypeStruct((peers, block, columns), BF16), limit=12)(
        mixed, gate_two, halo, conv_taps[1]
    )
    return finish(gated, out_weight)


def finish(gated, out_weight):
    peers, block, columns = gated.shape
    everyone = lax.all_to_all(gated, "col", 0, 0, tiled=True)
    weight = out_weight.reshape(peers, columns, -1)
    return jnp.einsum("crk,ckn->rn", everyone, weight, preferred_element_type=F32).astype(BF16)


def solution(mesh):
    spread_rows = ("grp", "row")
    in_specs = (
        P(spread_rows, "col"),
        P(spread_rows, "col"),
        P(spread_rows, "col"),
        P(None, None, "col"),
        P(),
        P(),
        P(),
        P(),
        P(),
        P(None, None, None, "col"),
        P(None, None, "col"),
        P(None, "col"),
        P(None, "col"),
    )
    return jax.shard_map(
        per_device, mesh=mesh, in_specs=in_specs, out_specs=P(spread_rows, "col"), check_vma=False
    )
```

```python
import functools
import math

import jax
import jax.numpy as jnp
import numpy as np
from jax import lax
from jax.experimental import pallas as pl
from jax.experimental.pallas import tpu as pltpu
from jax.sharding import PartitionSpec as P

ENERGY_FLOOR = 1.0
UNROLL = 8
F32 = jnp.float32
BF16 = jnp.bfloat16


def halves(value):
    high = value.astype(BF16)
    return high, (value - high.astype(F32)).astype(BF16)


def dot(left, right):
    return jnp.dot(left, right, preferred_element_type=F32)


def dot_wide(left_high, left_low, right_high, right_low):
    return dot(
        jnp.concatenate([left_high, left_low, left_high], 1),
        jnp.concatenate([right_high, right_high, right_low], 0),
    )


def cos_turns(turns):
    near = turns - jnp.round(turns)
    quarter = jnp.abs(near) - 0.25
    square = quarter * quarter
    total = jnp.full_like(square, SINE[-1])
    for factor in SINE[-2::-1]:
        total = total * square + factor
    return total * quarter


def fit_sine():
    nodes = 0.25 * np.cos(np.pi * (np.arange(64) + 0.5) / 128)
    powers = np.stack([nodes ** (2 * i + 1) for i in range(4)], 1)
    return [float(v) for v in np.linalg.lstsq(powers, -np.sin(2 * np.pi * nodes), rcond=None)[0]]


SINE = fit_sine()


def split_constant(table):
    high = table.astype(np.float32).astype(jnp.bfloat16)
    return np.stack([high, (table - high.astype(np.float64)).astype(np.float32).astype(jnp.bfloat16)])


@functools.lru_cache
def tables(rows, chan, block):
    waves = 2 * rows
    half = np.arange(rows + 1)
    phase = 2 * np.pi * (half[:, None] * np.arange(rows)[None] % waves) / waves
    weight = np.where((half == 0) | (half == rows), 1.0, 2.0)[:, None] / (waves * block)
    eye = np.eye(chan)
    into = np.concatenate([np.kron(np.cos(phase), eye), np.kron(-np.sin(phase[1:-1]), eye)])
    back = np.concatenate(
        [np.kron(weight * np.cos(phase), eye), np.kron(-(weight * np.sin(phase))[1:-1], eye)]
    ).T
    inner = 2 * np.pi * (np.arange(block)[:, None] * np.arange(block)[None] % block) / block
    pair = np.concatenate([np.cos(inner), np.sin(inner)], 0)
    turn = 2 * np.pi * half[:, None] * np.arange(block)[None] / (waves * block)
    twiddle = np.stack([np.cos(turn), np.sin(turn)]).astype(np.float32)
    return split_constant(into), split_constant(back), split_constant(pair), twiddle


def spread(twiddle_ref, part, chan):
    value = twiddle_ref[part]
    return jnp.broadcast_to(value[:, None, :], (value.shape[0], chan, value.shape[1])).reshape(-1, value.shape[1])


def first_stage(field, into_ref, chan):
    edge = field.shape[0] + chan
    high, low = halves(field)
    part_re = dot_wide(into_ref[0, :edge], into_ref[1, :edge], high, low)
    part_im = dot_wide(into_ref[0, edge:], into_ref[1, edge:], high, low)
    zero = jnp.zeros((chan, field.shape[1]), F32)
    return part_re, jnp.concatenate([zero, part_im, zero], 0)


def pair_product(first, second, pair_ref):
    first_high, first_low = halves(first)
    second_high, second_low = halves(second)
    return dot_wide(
        jnp.concatenate([first_high, second_high], 1),
        jnp.concatenate([first_low, second_low], 1),
        pair_ref[0],
        pair_ref[1],
    )


def forward(field, into_ref, pair_ref, cos_part, sin_part, chan):
    part_re, part_im = first_stage(field, into_ref, chan)
    turned_re = part_re * cos_part + part_im * sin_part
    turned_im = part_im * cos_part - part_re * sin_part
    return pair_product(turned_re, turned_im, pair_ref), pair_product(turned_im, -turned_re, pair_ref)


def backward(part_re, part_im, back_ref, pair_ref, cos_part, sin_part, chan):
    edge = part_re.shape[0]
    wave_re = pair_product(part_re, -part_im, pair_ref)
    wave_im = pair_product(part_im, part_re, pair_ref)
    turned_re = wave_re * cos_part - wave_im * sin_part
    turned_im = wave_re * sin_part + wave_im * cos_part
    high, low = halves(jnp.concatenate([turned_re, turned_im[chan : edge - chan]], 0))
    middle = back_ref.shape[1] // 2
    return jnp.concatenate(
        [
            dot_wide(back_ref[0, :middle], back_ref[1, :middle], high, low),
            dot_wide(back_ref[0, middle:], back_ref[1, middle:], high, low),
        ],
        0,
    )


def filter_kernel(
    rows, chan, one, embed_ref, first_bias_ref, freq_ref, inner_ref, second_bias_ref, weight_ref, decay_ref,
    band_ref, into_ref, pair_ref, twiddle_ref, spec_re_ref, spec_im_ref,
    first_table, second_table, taps_ref, energy_ref, near_ref, far_ref, first_w, second_w, last_w,
):
    block = taps_ref.shape[2]
    hidden = freq_ref.shape[1]
    seq_len = rows * block
    freq = freq_ref[...] * (0.5 / math.pi)
    second_bias = second_bias_ref[...] * freq - 0.25
    spare = lax.broadcasted_iota(jnp.int32, embed_ref.shape, 0) == one
    first_bias = first_bias_ref[...] * freq - 0.25
    w_one, w_two = halves(jnp.where(spare, first_bias, embed_ref[...] * freq))
    first_w[...] = jnp.concatenate([w_one, w_one, w_two, jnp.zeros_like(w_two)], 0)
    v_one, v_two = halves(inner_ref[...] * freq)
    second_w[:, :hidden] = jnp.concatenate([v_one, v_one], 0)
    second_w[:, hidden:] = jnp.concatenate([v_two, v_two], 0)
    u_one, u_two = halves(weight_ref[...])
    last_w[:, :hidden] = jnp.concatenate([u_one, u_two], 0)
    last_w[:, hidden:] = jnp.concatenate([u_one, jnp.zeros_like(u_two)], 0)
    band = band_ref[0:1]
    shift = band_ref[1:2]
    line = band_ref[2:3]
    lag = lax.broadcasted_iota(jnp.int32, (block, 2 * embed_ref.shape[0]), 0).astype(F32)
    turns = lag * band * (1.0 / seq_len)
    first_table[...] = jnp.where(line > 0, 1.0, cos_turns(turns + shift))
    second_table[...] = jnp.where(line > 0, lag * (1.0 / seq_len), cos_turns(turns + (shift + 0.25)))
    start = lax.broadcasted_iota(jnp.int32, (rows, 2 * embed_ref.shape[0]), 0).astype(F32)
    turns = start * band * (1.0 / rows)
    near_ref[...] = jnp.where(line > 0, start * (1.0 / rows), cos_turns(turns))
    far_ref[...] = jnp.where(line > 0, 1.0, cos_turns(turns - 0.25))
    energy_ref[...] = jnp.zeros_like(energy_ref)
    decay = decay_ref[...]
    lanes = lax.broadcasted_iota(jnp.int32, (1, block), 1)
    left = lax.broadcasted_iota(jnp.int32, (1, 2 * embed_ref.shape[0]), 1) < embed_ref.shape[0]
    parts = weight_ref.shape[0]
    is_back = (lax.broadcasted_iota(jnp.int32, (parts, 1), 0) // chan) % 2 == 1

    def lags(row):
        feature = first_table[...] * near_ref[pl.ds(row, 1), :] + second_table[...] * far_ref[pl.ds(row, 1), :]
        x_one, x_two = halves(feature)
        layer_one = cos_turns(dot(jnp.concatenate([jnp.where(left, x_one, x_two), x_one], 1), first_w[...]))
        y_one, y_two = halves(layer_one)
        both = dot(jnp.concatenate([y_one, y_two], 1), second_w[...])
        layer_two = cos_turns(both[:, :hidden] + both[:, hidden:] + second_bias)
        z_one, z_two = halves(layer_two)
        both = lax.dot_general(
            last_w[...], jnp.concatenate([z_one, z_two], 1), (((1,), (1,)), ((), ())), preferred_element_type=F32
        )
        raw = both[:parts] + both[parts:]
        at = lanes + row * block
        taps = raw * jnp.exp(decay * (at.astype(F32) * (-1.0 / seq_len)))
        return jnp.where(is_back & (at == 0), 0.0, taps)

    @pl.loop(0, rows // UNROLL)
    def _(step):
        found = [lags(UNROLL * step + k) for k in range(UNROLL)]
        energy_ref[...] += sum(taps * taps for taps in found)
        for k in range(UNROLL):
            place = pl.multiple_of((UNROLL * step + k) * chan, chan)
            for order in range(parts // (2 * chan)):
                base = order * 2 * chan
                ahead = found[k][base : base + chan]
                behind = found[k][base + chan : base + 2 * chan]
                taps_ref[2 * order, pl.ds(place, chan), :] = ahead + behind
                taps_ref[2 * order + 1, pl.ds(place, chan), :] = ahead - behind

    total = jnp.sum(energy_ref[...], axis=1, keepdims=True)
    cos_part, sin_part = spread(twiddle_ref, 0, chan), spread(twiddle_ref, 1, chan)
    for order in range(parts // (2 * chan)):
        base = order * 2 * chan
        scale = lax.rsqrt(total[base : base + chan] + total[base + chan : base + 2 * chan] + ENERGY_FLOOR)
        scale = jnp.broadcast_to(scale[None], (rows + 1, chan, block)).reshape(-1, block)
        even_re, even_im = first_stage(taps_ref[2 * order], into_ref, chan)
        odd_re, odd_im = first_stage(taps_ref[2 * order + 1], into_ref, chan)
        spec_re_ref[order] = scale * pair_product(
            even_re * cos_part + even_im * sin_part, even_im * cos_part - even_re * sin_part, pair_ref
        )
        spec_im_ref[order] = scale * pair_product(
            odd_im * cos_part - odd_re * sin_part, -(odd_re * cos_part + odd_im * sin_part), pair_ref
        )


def short(signal, taps, first, rows, chan):
    block = signal.shape[1]
    lanes = lax.broadcasted_iota(jnp.int32, signal.shape, 1)
    line = lax.broadcasted_iota(jnp.int32, signal.shape, 0)
    size = signal.shape[0]
    before = pltpu.roll(signal, 1, 1)
    crossed = jnp.where(line < chan, 0.0, pltpu.roll(before, chan, 0))
    before = jnp.where(lanes == 0, crossed, before)
    after = pltpu.roll(signal, block - 1, 1)
    crossed = jnp.where(line >= size - chan, 0.0, pltpu.roll(after, size - chan, 0))
    after = jnp.where(lanes == block - 1, crossed, after)

    def tap(k):
        column = taps[:, first + k : first + k + 1]
        return jnp.broadcast_to(column[None], (rows, chan, block)).reshape(size, block)

    return before * tap(0) + signal * tap(1) + after * tap(2)


def conv_kernel(
    rows, chan, orders, arrived_ref, param_ref, spec_re_ref, spec_im_ref, into_ref, back_ref, pair_ref,
    twiddle_ref, out_ref,
):
    block = arrived_ref.shape[2]
    size = rows * chan
    param = param_ref[...]

    def signal(k):
        return arrived_ref[:, k * chan : (k + 1) * chan, :].astype(F32).reshape(size, block)

    cos_part, sin_part = spread(twiddle_ref, 0, chan), spread(twiddle_ref, 1, chan)
    current = short(signal(0), param, 6, rows, chan)
    for order in range(orders):
        data_re, data_im = forward(current, into_ref, pair_ref, cos_part, sin_part, chan)
        spec_re, spec_im = spec_re_ref[order], spec_im_ref[order]
        long_part = backward(
            data_re * spec_re - data_im * spec_im,
            data_re * spec_im + data_im * spec_re,
            back_ref, pair_ref, cos_part, sin_part, chan,
        )
        column = param[:, 9 + order : 10 + order]
        skip = jnp.broadcast_to(column[None], (rows, chan, block)).reshape(size, block)
        current = long_part + skip * current
        if order < orders - 1:
            current = current * short(signal(order + 1), param, 3 * order, rows, chan)
    out_ref[...] = current.astype(BF16).reshape(rows, chan, block)


def turn_kernel(first_ref, second_ref, out_ref):
    rows = out_ref.shape[0]
    chan = out_ref.shape[1] // 2
    for k, ref in enumerate((first_ref, second_ref)):
        turned = jnp.transpose(ref[...].astype(F32)).astype(BF16)
        out_ref[:, k * chan : (k + 1) * chan, :] = turned.reshape(rows, chan, -1)


def gate_kernel(mixed_ref, gate_ref, halo_ref, taps_ref, out_ref):
    gate = gate_ref[...].astype(F32)
    block = gate.shape[0]
    line = lax.broadcasted_iota(jnp.int32, gate.shape, 0)
    halo = halo_ref[...].astype(F32)
    taps = taps_ref[...].astype(F32)
    before = jnp.where(line == 0, halo[0:1], pltpu.roll(gate, 1, 0))
    after = jnp.where(line == block - 1, halo[1:2], pltpu.roll(gate, block - 1, 0))
    factor = before * taps[0:1] + gate * taps[1:2] + after * taps[2:3]
    gated = (jnp.transpose(mixed_ref[...].astype(F32)) * factor).astype(BF16)
    for peer in range(out_ref.shape[0]):
        out_ref[peer] = gated


def call(kernel, out_shape, scratch=(), flops=0, grant=None):
    return pl.pallas_call(
        kernel,
        out_shape=out_shape,
        scratch_shapes=scratch,
        cost_estimate=pl.CostEstimate(flops=flops, bytes_accessed=0, transcendentals=0),
        compiler_params=pltpu.CompilerParams(vmem_limit_bytes=grant),
    )


def per_device(
    gate_one, gate_two, values, conv_taps, embed_weight, embed_bias, sine_freq, inner_weight, inner_bias,
    filter_weight, decay_rate, skip_gain, out_weight,
):
    rows = lax.axis_size("row")
    own = lax.axis_index("row")
    block, columns = gate_one.shape
    orders = skip_gain.shape[0]
    chan = columns // rows
    offset = own * chan
    hidden = sine_freq.shape[0]
    features = embed_weight.shape[0]
    peers = lax.axis_size("col")
    bands = (features - 1) // 2
    into, back, pair, twiddle = tables(rows, chan, block)

    turned = call(turn_kernel, jax.ShapeDtypeStruct((rows, 2 * chan, block), BF16))(values, gate_one)
    arrived = lax.all_to_all(turned, "row", 0, 0, tiled=True)

    down = [(k, k + 1) for k in range(rows - 1)]
    up = [(k + 1, k) for k in range(rows - 1)]
    halo = jnp.concatenate(
        [lax.ppermute(gate_two[-1:], "row", down), lax.ppermute(gate_two[:1], "row", up)], 0
    )

    weight_here = lax.dynamic_slice_in_dim(filter_weight, offset, chan, 3)
    weight_here = jnp.transpose(weight_here.reshape(hidden, -1))
    decay_here = lax.dynamic_slice_in_dim(decay_rate, offset, chan, 2).reshape(-1, 1)
    taps_here = lax.dynamic_slice_in_dim(conv_taps, offset, chan, 2).astype(F32).reshape(-1, chan)
    skip_here = lax.dynamic_slice_in_dim(skip_gain, offset, chan, 1)
    param = jnp.transpose(jnp.concatenate([taps_here, skip_here], 0))

    width = 64
    embed = jnp.pad(embed_weight, ((0, width - features), (0, 0)))
    steps = np.linspace(0.0001, bands - 1, bands).astype(np.float32)
    band = np.zeros((3, width), np.float32)
    band[0, 1:features] = np.concatenate([steps, steps])
    band[1, 1 + bands : features] = 0.25
    band[2, 0] = 1
    band[:, features:] = 0
    band = np.concatenate([band, band], 1)

    edge = (rows + 1) * chan
    parts = weight_here.shape[0]
    spec_shape = jax.ShapeDtypeStruct((orders, edge, block), F32)
    spec_re, spec_im = call(
        functools.partial(filter_kernel, rows, chan, features),
        (spec_shape, spec_shape),
        (
            pltpu.VMEM((block, 2 * width), F32),
            pltpu.VMEM((block, 2 * width), F32),
            pltpu.VMEM((parts // chan, rows * chan, block), F32),
            pltpu.VMEM((parts, block), F32),
            pltpu.VMEM((rows, 2 * width), F32),
            pltpu.VMEM((rows, 2 * width), F32),
            pltpu.VMEM((4 * width, hidden), BF16),
            pltpu.VMEM((2 * hidden, 2 * hidden), BF16),
            pltpu.VMEM((2 * parts, 2 * hidden), BF16),
        ),
        flops=12_000_000_000,
    )(
        embed, embed_bias[None], sine_freq[None], inner_weight, inner_bias[None], weight_here, decay_here,
        band, into, pair, twiddle,
    )
    mixed = call(
        functools.partial(conv_kernel, rows, chan, orders),
        jax.ShapeDtypeStruct((rows, chan, block), BF16),
        flops=5_000_000_000,
    )(arrived, param, spec_re, spec_im, into, back, pair, twiddle)
    mixed = lax.all_to_all(mixed, "row", 0, 0, tiled=True).reshape(columns, block)
    gated = call(gate_kernel, jax.ShapeDtypeStruct((peers, block, columns), BF16), grant=12 << 20)(
        mixed, gate_two, halo, conv_taps[1]
    )
    return finish(gated, out_weight)


def finish(gated, out_weight):
    peers, block, columns = gated.shape
    everyone = lax.all_to_all(gated, "col", 0, 0, tiled=True)
    weight = out_weight.reshape(peers, columns, -1)
    return jnp.einsum("crk,ckn->rn", everyone, weight, preferred_element_type=F32).astype(BF16)


def solution(mesh):
    spread_rows = ("grp", "row")
    in_specs = (
        P(spread_rows, "col"),
        P(spread_rows, "col"),
        P(spread_rows, "col"),
        P(None, None, "col"),
        P(),
        P(),
        P(),
        P(),
        P(),
        P(None, None, None, "col"),
        P(None, None, "col"),
        P(None, "col"),
        P(None, "col"),
    )
    return jax.shard_map(
        per_device, mesh=mesh, in_specs=in_specs, out_specs=P(spread_rows, "col"), check_vma=False
    )
```

```python
import functools
import math

import jax
import jax.numpy as jnp
import numpy as np
from jax import lax
from jax.experimental import pallas as pl
from jax.experimental.pallas import tpu as pltpu
from jax.sharding import PartitionSpec as P


ENERGY_FLOOR = 1.0
UNROLL = 8
GRANT = 60
F32 = jnp.float32
BF16 = jnp.bfloat16


def halves(value):
    high = value.astype(BF16)
    return high, (value - high.astype(F32)).astype(BF16)


def thirds(value):
    high = value.astype(BF16)
    rest = value - high.astype(F32)
    middle = rest.astype(BF16)
    return high, middle, (rest - middle.astype(F32)).astype(BF16)


def dot(left, right):
    return jnp.dot(left, right, preferred_element_type=F32)


def dot_wide(left_high, left_low, right_high, right_low):
    return dot(
        jnp.concatenate([left_high, left_low, left_high], 1),
        jnp.concatenate([right_high, right_high, right_low], 0),
    )


def cos_turns(turns):
    near = turns - jnp.round(turns)
    quarter = jnp.abs(near) - 0.25
    square = quarter * quarter
    total = jnp.full_like(square, SINE[-1])
    for factor in SINE[-2::-1]:
        total = total * square + factor
    return total * quarter


def fit_sine():
    nodes = 0.25 * np.cos(np.pi * (np.arange(64) + 0.5) / 128)
    powers = np.stack([nodes ** (2 * i + 1) for i in range(4)], 1)
    return [float(v) for v in np.linalg.lstsq(powers, -np.sin(2 * np.pi * nodes), rcond=None)[0]]


SINE = fit_sine()


def split_constant(table):
    high = table.astype(np.float32).astype(jnp.bfloat16)
    return np.stack([high, (table - high.astype(np.float64)).astype(np.float32).astype(jnp.bfloat16)])


@functools.lru_cache
def tables(rows, chan, block):
    waves = 2 * rows
    half = np.arange(rows + 1)
    phase = 2 * np.pi * (half[:, None] * np.arange(rows)[None] % waves) / waves
    weight = np.where((half == 0) | (half == rows), 1.0, 2.0)[:, None] / (waves * block)
    eye = np.eye(chan)
    into = np.concatenate([np.kron(np.cos(phase), eye), np.kron(-np.sin(phase[1:-1]), eye)])
    back = np.concatenate(
        [np.kron(weight * np.cos(phase), eye), np.kron(-(weight * np.sin(phase))[1:-1], eye)]
    ).T
    inner = 2 * np.pi * (np.arange(block)[:, None] * np.arange(block)[None] % block) / block
    pair = np.concatenate([np.cos(inner), np.sin(inner)], 0)
    turn = 2 * np.pi * half[:, None] * np.arange(block)[None] / (waves * block)
    twiddle = np.stack([np.cos(turn), np.sin(turn)]).astype(np.float32)
    return split_constant(into), split_constant(back), split_constant(pair), twiddle


def spread(twiddle_ref, part, chan):
    value = twiddle_ref[part]
    return jnp.broadcast_to(value[:, None, :], (value.shape[0], chan, value.shape[1])).reshape(-1, value.shape[1])


def first_stage(field, into_ref, chan):
    edge = field.shape[0] + chan
    high, low = halves(field)
    part_re = dot_wide(into_ref[0, :edge], into_ref[1, :edge], high, low)
    part_im = dot_wide(into_ref[0, edge:], into_ref[1, edge:], high, low)
    zero = jnp.zeros((chan, field.shape[1]), F32)
    return part_re, jnp.concatenate([zero, part_im, zero], 0)


def pair_product(first, second, pair_ref):
    first_high, first_low = halves(first)
    second_high, second_low = halves(second)
    return dot_wide(
        jnp.concatenate([first_high, second_high], 1),
        jnp.concatenate([first_low, second_low], 1),
        pair_ref[0],
        pair_ref[1],
    )


def forward(field, into_ref, pair_ref, cos_part, sin_part, chan):
    part_re, part_im = first_stage(field, into_ref, chan)
    turned_re = part_re * cos_part + part_im * sin_part
    turned_im = part_im * cos_part - part_re * sin_part
    return pair_product(turned_re, turned_im, pair_ref), pair_product(turned_im, -turned_re, pair_ref)


def backward(part_re, part_im, back_ref, pair_ref, cos_part, sin_part, chan):
    edge = part_re.shape[0]
    wave_re = pair_product(part_re, -part_im, pair_ref)
    wave_im = pair_product(part_im, part_re, pair_ref)
    turned_re = wave_re * cos_part - wave_im * sin_part
    turned_im = wave_re * sin_part + wave_im * cos_part
    high, low = halves(jnp.concatenate([turned_re, turned_im[chan : edge - chan]], 0))
    middle = back_ref.shape[1] // 2
    return jnp.concatenate(
        [
            dot_wide(back_ref[0, :middle], back_ref[1, :middle], high, low),
            dot_wide(back_ref[0, middle:], back_ref[1, middle:], high, low),
        ],
        0,
    )


def filter_kernel(
    rows, chan, embed_ref, first_bias_ref, freq_ref, inner_ref, second_bias_ref, weight_ref, decay_ref, conv_taps_ref,
    skip_ref, halo_ref, band_ref, into_ref, pair_ref, twiddle_ref, spec_re_ref, spec_im_ref, param_ref,
    first_table, second_table, taps_ref, energy_ref, near_ref, far_ref, embed, first_w, second_w, last_w,
    into, pair, arrivals,
):
    fetches = [
        pltpu.make_async_copy(source, target, arrivals.at[k])
        for k, (source, target) in enumerate(((into_ref, into), (pair_ref, pair)))
    ]
    for fetch in fetches:
        fetch.start()
    del halo_ref
    block = taps_ref.shape[2]
    hidden = freq_ref.shape[1]
    seq_len = rows * block
    orders = skip_ref.shape[0]
    parts = 2 * orders * chan
    width = embed.shape[0]
    columns = skip_ref.shape[1]
    freq = freq_ref[...] * (0.5 / math.pi)
    second_bias = second_bias_ref[...] * freq - 0.25
    count = embed_ref.shape[0]
    embed[...] = jnp.zeros_like(embed)
    embed[:count, :] = embed_ref[...] * freq
    embed[count : count + 1, :] = first_bias_ref[...] * freq - 0.25
    w_one, w_two = halves(embed[...])
    first_w[...] = jnp.concatenate([w_one, w_one, w_two, jnp.zeros_like(w_two)], 0)
    v_one, v_two = halves(inner_ref[...] * freq)
    second_w[:, :hidden] = jnp.concatenate([v_one, v_one], 0)
    second_w[:, hidden:] = jnp.concatenate([v_two, v_two], 0)
    place = lax.broadcasted_iota(jnp.int32, (chan, columns), 1) - lax.axis_index("row") * chan
    chosen = (place == lax.broadcasted_iota(jnp.int32, (chan, columns), 0)).astype(F32).astype(BF16)

    def choose(table):
        return lax.dot_general(chosen, table, (((1,), (1,)), ((), ())), preferred_element_type=F32)

    def choose_exactly(table):
        return sum(choose(part) for part in thirds(table))

    for k in range(2 * orders):
        u_one, u_two = (
            choose(part).astype(BF16) for part in halves(weight_ref[k // 2, k % 2])
        )
        last_w[k * chan : (k + 1) * chan, :] = jnp.concatenate([u_one, u_one], 1)
        last_w[parts + k * chan : parts + (k + 1) * chan, :] = jnp.concatenate([u_two, jnp.zeros_like(u_two)], 1)
    decay = []
    for order in range(orders):
        here = choose_exactly(decay_ref[order])
        decay += [here[:, 0:1], here[:, 1:2]]
    decay = jnp.concatenate(decay, 0)
    for k in range(conv_taps_ref.shape[0]):
        param_ref[k, :, 0:3] = choose(conv_taps_ref[k])
    param_ref[conv_taps_ref.shape[0], :, 0:orders] = choose_exactly(skip_ref[...])
    band = band_ref[0:1]
    shift = band_ref[1:2]
    line = band_ref[2:3]
    lag = lax.broadcasted_iota(jnp.int32, (block, 2 * width), 0).astype(F32)
    turns = lag * band * (1.0 / seq_len)
    first_table[...] = jnp.where(line > 0, 1.0, cos_turns(turns + shift))
    second_table[...] = jnp.where(line > 0, lag * (1.0 / seq_len), cos_turns(turns + (shift + 0.25)))
    start = lax.broadcasted_iota(jnp.int32, (rows, 2 * width), 0).astype(F32)
    turns = start * band * (1.0 / rows)
    near_ref[...] = jnp.where(line > 0, start * (1.0 / rows), cos_turns(turns))
    far_ref[...] = jnp.where(line > 0, 1.0, cos_turns(turns - 0.25))
    energy_ref[...] = jnp.zeros_like(energy_ref)
    lanes = lax.broadcasted_iota(jnp.int32, (1, block), 1)
    left = lax.broadcasted_iota(jnp.int32, (1, 2 * width), 1) < width
    is_back = (lax.broadcasted_iota(jnp.int32, (parts, 1), 0) // chan) % 2 == 1

    def lags(row):
        feature = first_table[...] * near_ref[pl.ds(row, 1), :] + second_table[...] * far_ref[pl.ds(row, 1), :]
        x_one, x_two = halves(feature)
        layer_one = cos_turns(dot(jnp.concatenate([jnp.where(left, x_one, x_two), x_one], 1), first_w[...]))
        y_one, y_two = halves(layer_one)
        both = dot(jnp.concatenate([y_one, y_two], 1), second_w[...])
        layer_two = cos_turns(both[:, :hidden] + both[:, hidden:] + second_bias)
        z_one, z_two = halves(layer_two)
        both = lax.dot_general(
            last_w[...], jnp.concatenate([z_one, z_two], 1), (((1,), (1,)), ((), ())), preferred_element_type=F32
        )
        raw = both[:parts] + both[parts:]
        at = lanes + row * block
        taps = raw * jnp.exp(decay * (at.astype(F32) * (-1.0 / seq_len)))
        return jnp.where(is_back & (at == 0), 0.0, taps)

    @pl.loop(0, rows // UNROLL)
    def _(step):
        found = [lags(UNROLL * step + k) for k in range(UNROLL)]
        energy_ref[...] += sum(taps * taps for taps in found)
        for k in range(UNROLL):
            place = pl.multiple_of((UNROLL * step + k) * chan, chan)
            for order in range(parts // (2 * chan)):
                base = order * 2 * chan
                ahead = found[k][base : base + chan]
                behind = found[k][base + chan : base + 2 * chan]
                taps_ref[2 * order, pl.ds(place, chan), :] = ahead + behind
                taps_ref[2 * order + 1, pl.ds(place, chan), :] = ahead - behind

    for fetch in fetches:
        fetch.wait()
    total = jnp.sum(energy_ref[...], axis=1, keepdims=True)
    cos_part, sin_part = spread(twiddle_ref, 0, chan), spread(twiddle_ref, 1, chan)
    for order in range(parts // (2 * chan)):
        base = order * 2 * chan
        scale = lax.rsqrt(total[base : base + chan] + total[base + chan : base + 2 * chan] + ENERGY_FLOOR)
        scale = jnp.broadcast_to(scale[None], (rows + 1, chan, block)).reshape(-1, block)
        even_re, even_im = first_stage(taps_ref[2 * order], into, chan)
        odd_re, odd_im = first_stage(taps_ref[2 * order + 1], into, chan)
        spec_re_ref[order] = scale * pair_product(
            even_re * cos_part + even_im * sin_part, even_im * cos_part - even_re * sin_part, pair
        )
        spec_im_ref[order] = scale * pair_product(
            odd_im * cos_part - odd_re * sin_part, -(odd_re * cos_part + odd_im * sin_part), pair
        )


def short(signal, taps, rows, chan):
    block = signal.shape[1]
    lanes = lax.broadcasted_iota(jnp.int32, signal.shape, 1)
    line = lax.broadcasted_iota(jnp.int32, signal.shape, 0)
    size = signal.shape[0]
    before = pltpu.roll(signal, 1, 1)
    crossed = jnp.where(line < chan, 0.0, pltpu.roll(before, chan, 0))
    before = jnp.where(lanes == 0, crossed, before)
    after = pltpu.roll(signal, block - 1, 1)
    crossed = jnp.where(line >= size - chan, 0.0, pltpu.roll(after, size - chan, 0))
    after = jnp.where(lanes == block - 1, crossed, after)

    def tap(k):
        column = taps[:, k : k + 1]
        return jnp.broadcast_to(column[None], (rows, chan, block)).reshape(size, block)

    return before * tap(0) + signal * tap(1) + after * tap(2)


def conv_kernel(
    rows, chan, orders, arrived_ref, param_ref, into_ref, twiddle_ref, pair_ref, spec_re_ref, spec_im_ref, back_ref,
    out_ref, into, twiddle, pair, spec_re, spec_im, back, arrivals,
):
    sources = (into_ref, twiddle_ref, pair_ref, spec_re_ref, spec_im_ref, back_ref)
    targets = (into, twiddle, pair, spec_re, spec_im, back)
    fetches = [
        pltpu.make_async_copy(source, target, arrivals.at[k])
        for k, (source, target) in enumerate(zip(sources, targets))
    ]
    for fetch in fetches:
        fetch.start()
    block = arrived_ref.shape[2]
    size = rows * chan

    def signal(k):
        return arrived_ref[:, k * chan : (k + 1) * chan, :].astype(F32).reshape(size, block)

    current = short(signal(0), param_ref[orders], rows, chan)
    for fetch in fetches:
        fetch.wait()
    cos_part, sin_part = spread(twiddle, 0, chan), spread(twiddle, 1, chan)
    for order in range(orders):
        data_re, data_im = forward(current, into, pair, cos_part, sin_part, chan)
        own_re, own_im = spec_re[order], spec_im[order]
        long_part = backward(
            data_re * own_re - data_im * own_im,
            data_re * own_im + data_im * own_re,
            back, pair, cos_part, sin_part, chan,
        )
        column = param_ref[orders + 1, :, order : order + 1]
        skip = jnp.broadcast_to(column[None], (rows, chan, block)).reshape(size, block)
        current = long_part + skip * current
        if order < orders - 1:
            current = current * short(signal(order + 1), param_ref[order], rows, chan)
    out_ref[...] = current.astype(BF16).reshape(rows, chan, block)


def turn_kernel(first_ref, second_ref, out_ref):
    rows = out_ref.shape[0]
    chan = out_ref.shape[1] // 2
    for k, ref in enumerate((first_ref, second_ref)):
        turned = jnp.transpose(ref[...].astype(F32)).astype(BF16)
        out_ref[:, k * chan : (k + 1) * chan, :] = turned.reshape(rows, chan, -1)


def gate_kernel(mixed_ref, gate_ref, halo_ref, taps_ref, out_ref):
    gate = gate_ref[...].astype(F32)
    block = gate.shape[0]
    line = lax.broadcasted_iota(jnp.int32, gate.shape, 0)
    halo = halo_ref[...].astype(F32)
    taps = taps_ref[...].astype(F32)
    before = jnp.where(line == 0, halo[0:1], pltpu.roll(gate, 1, 0))
    after = jnp.where(line == block - 1, halo[1:2], pltpu.roll(gate, block - 1, 0))
    factor = before * taps[0:1] + gate * taps[1:2] + after * taps[2:3]
    gated = (jnp.transpose(mixed_ref[...].astype(F32)) * factor).astype(BF16)
    for peer in range(out_ref.shape[0]):
        out_ref[peer] = gated


def call(kernel, out_shape, scratch=(), flops=0, grant=None, placed=None):
    specs = {} if placed is None else {"in_specs": [pl.BlockSpec(memory_space=space) for space in placed]}
    return pl.pallas_call(
        kernel,
        out_shape=out_shape,
        **specs,
        scratch_shapes=scratch,
        cost_estimate=pl.CostEstimate(flops=flops, bytes_accessed=0, transcendentals=0),
        compiler_params=pltpu.CompilerParams(vmem_limit_bytes=grant),
    )


def per_device(
    gate_one, gate_two, values, conv_taps, embed_weight, embed_bias, sine_freq, inner_weight, inner_bias,
    filter_weight, decay_rate, skip_gain, out_weight,
):
    rows = lax.axis_size("row")
    block, columns = gate_one.shape
    orders = skip_gain.shape[0]
    chan = columns // rows
    hidden = sine_freq.shape[0]
    features = embed_weight.shape[0]
    peers = lax.axis_size("col")
    bands = (features - 1) // 2
    into, back, pair, twiddle = tables(rows, chan, block)

    turned = call(turn_kernel, jax.ShapeDtypeStruct((rows, 2 * chan, block), BF16))(values, gate_one)
    arrived = lax.all_to_all(turned, "row", 0, 0, tiled=True)

    down = [(k, k + 1) for k in range(rows - 1)]
    up = [(k + 1, k) for k in range(rows - 1)]
    halo = [lax.ppermute(gate_two[-1:], "row", down), lax.ppermute(gate_two[:1], "row", up)]
    halo = jnp.concatenate(halo, 0)

    width = 64
    steps = np.linspace(0.0001, bands - 1, bands).astype(np.float32)
    band = np.zeros((3, width), np.float32)
    band[0, 1:features] = np.concatenate([steps, steps])
    band[1, 1 + bands : features] = 0.25
    band[2, 0] = 1
    band[:, features:] = 0
    band = np.concatenate([band, band], 1)

    edge = (rows + 1) * chan
    parts = 2 * orders * chan
    spec_shape = jax.ShapeDtypeStruct((orders, edge, block), F32)
    vmem, anywhere = pltpu.VMEM, pl.ANY
    spec_re, spec_im, param = call(
        functools.partial(filter_kernel, rows, chan),
        (spec_shape, spec_shape, jax.ShapeDtypeStruct((conv_taps.shape[0] + 1, chan, 4), F32)),
        (
            pltpu.VMEM((block, 2 * width), F32),
            pltpu.VMEM((block, 2 * width), F32),
            pltpu.VMEM((parts // chan, rows * chan, block), F32),
            pltpu.VMEM((parts, block), F32),
            pltpu.VMEM((rows, 2 * width), F32),
            pltpu.VMEM((rows, 2 * width), F32),
            pltpu.VMEM((width, hidden), F32),
            pltpu.VMEM((4 * width, hidden), BF16),
            pltpu.VMEM((2 * hidden, 2 * hidden), BF16),
            pltpu.VMEM((2 * parts, 2 * hidden), BF16),
            pltpu.VMEM(into.shape, BF16),
            pltpu.VMEM(pair.shape, BF16),
            pltpu.SemaphoreType.DMA((2,)),
        ),
        flops=12_000_000_000,
        placed=[vmem] * 11 + [anywhere] * 2 + [vmem],
    )(
        embed_weight, embed_bias[None], sine_freq[None], inner_weight, inner_bias[None],
        jnp.transpose(filter_weight, (1, 2, 0, 3)), decay_rate, conv_taps, skip_gain, halo, band, into, pair, twiddle,
    )
    fetched = (into, twiddle, pair, spec_re, spec_im, back)
    mixed = call(
        functools.partial(conv_kernel, rows, chan, orders),
        jax.ShapeDtypeStruct((rows, chan, block), BF16),
        [*(pltpu.VMEM(table.shape, table.dtype) for table in fetched), pltpu.SemaphoreType.DMA((len(fetched),))],
        flops=5_000_000_000,
        grant=GRANT << 20,
        placed=[vmem] * 2 + [anywhere] * len(fetched),
    )(arrived, param, *fetched)
    mixed = lax.all_to_all(mixed, "row", 0, 0, tiled=True).reshape(columns, block)
    gated = call(gate_kernel, jax.ShapeDtypeStruct((peers, block, columns), BF16), grant=12 << 20)(
        mixed, gate_two, halo, conv_taps[1]
    )
    return finish(gated, out_weight)


def finish(gated, out_weight):
    peers, _, columns = gated.shape
    everyone = lax.all_to_all(gated, "col", 0, 0, tiled=True)
    weight = out_weight.reshape(peers, columns, -1)
    return jnp.einsum("crk,ckn->rn", everyone, weight, preferred_element_type=F32).astype(BF16)


def solution(mesh):
    spread_rows = ("grp", "row")
    in_specs = (
        P(spread_rows, "col"),
        P(spread_rows, "col"),
        P(spread_rows, "col"),
        P(None, None, "col"),
        P(),
        P(),
        P(),
        P(),
        P(),
        P(None, None, None, "col"),
        P(None, None, "col"),
        P(None, "col"),
        P(None, "col"),
    )
    return jax.shard_map(
        per_device, mesh=mesh, in_specs=in_specs, out_specs=P(spread_rows, "col"), check_vma=False
    )
```

```python
import functools
import math

import jax
import jax.numpy as jnp
import numpy as np
from jax import lax
from jax.experimental import pallas as pl
from jax.experimental.pallas import tpu as pltpu
from jax.sharding import PartitionSpec as P

ENERGY_FLOOR = 1.0
UNROLL = 8
F32 = jnp.float32
BF16 = jnp.bfloat16


def halves(value):
    high = value.astype(BF16)
    return high, (value - high.astype(F32)).astype(BF16)


def thirds(value):
    high = value.astype(BF16)
    rest = value - high.astype(F32)
    middle = rest.astype(BF16)
    return high, middle, (rest - middle.astype(F32)).astype(BF16)


def dot(left, right):
    return jnp.dot(left, right, preferred_element_type=F32)


def dot_wide(left_high, left_low, right_high, right_low):
    return dot(
        jnp.concatenate([left_high, left_low, left_high], 1),
        jnp.concatenate([right_high, right_high, right_low], 0),
    )


def cos_turns(turns):
    near = turns - jnp.round(turns)
    quarter = jnp.abs(near) - 0.25
    square = quarter * quarter
    total = jnp.full_like(square, SINE[-1])
    for factor in SINE[-2::-1]:
        total = total * square + factor
    return total * quarter


def fit_sine():
    nodes = 0.25 * np.cos(np.pi * (np.arange(64) + 0.5) / 128)
    powers = np.stack([nodes ** (2 * i + 1) for i in range(4)], 1)
    return [float(v) for v in np.linalg.lstsq(powers, -np.sin(2 * np.pi * nodes), rcond=None)[0]]


SINE = fit_sine()


def split_constant(table):
    high = table.astype(np.float32).astype(jnp.bfloat16)
    return np.stack([high, (table - high.astype(np.float64)).astype(np.float32).astype(jnp.bfloat16)])


@functools.lru_cache
def tables(rows, chan, block):
    waves = 2 * rows
    half = np.arange(rows + 1)
    phase = 2 * np.pi * (half[:, None] * np.arange(rows)[None] % waves) / waves
    weight = np.where((half == 0) | (half == rows), 1.0, 2.0)[:, None] / (waves * block)
    eye = np.eye(chan)
    into = np.concatenate([np.kron(np.cos(phase), eye), np.kron(-np.sin(phase[1:-1]), eye)])
    back = np.concatenate(
        [np.kron(weight * np.cos(phase), eye), np.kron(-(weight * np.sin(phase))[1:-1], eye)]
    ).T
    inner = 2 * np.pi * (np.arange(block)[:, None] * np.arange(block)[None] % block) / block
    pair = np.concatenate([np.cos(inner), np.sin(inner)], 0)
    turn = 2 * np.pi * half[:, None] * np.arange(block)[None] / (waves * block)
    twiddle = np.stack([np.cos(turn), np.sin(turn)]).astype(np.float32)
    return split_constant(into), split_constant(back), split_constant(pair), twiddle


def spread(twiddle_ref, part, chan):
    value = twiddle_ref[part]
    return jnp.broadcast_to(value[:, None, :], (value.shape[0], chan, value.shape[1])).reshape(-1, value.shape[1])


def first_stage(field, into_ref, chan):
    edge = field.shape[0] + chan
    high, low = halves(field)
    part_re = dot_wide(into_ref[0, :edge], into_ref[1, :edge], high, low)
    part_im = dot_wide(into_ref[0, edge:], into_ref[1, edge:], high, low)
    zero = jnp.zeros((chan, field.shape[1]), F32)
    return part_re, jnp.concatenate([zero, part_im, zero], 0)


def pair_product(first, second, pair_ref):
    first_high, first_low = halves(first)
    second_high, second_low = halves(second)
    return dot_wide(
        jnp.concatenate([first_high, second_high], 1),
        jnp.concatenate([first_low, second_low], 1),
        pair_ref[0],
        pair_ref[1],
    )


def forward(field, into_ref, pair_ref, cos_part, sin_part, chan):
    part_re, part_im = first_stage(field, into_ref, chan)
    turned_re = part_re * cos_part + part_im * sin_part
    turned_im = part_im * cos_part - part_re * sin_part
    return pair_product(turned_re, turned_im, pair_ref), pair_product(turned_im, -turned_re, pair_ref)


def backward(part_re, part_im, back_ref, pair_ref, cos_part, sin_part, chan):
    edge = part_re.shape[0]
    wave_re = pair_product(part_re, -part_im, pair_ref)
    wave_im = pair_product(part_im, part_re, pair_ref)
    turned_re = wave_re * cos_part - wave_im * sin_part
    turned_im = wave_re * sin_part + wave_im * cos_part
    high, low = halves(jnp.concatenate([turned_re, turned_im[chan : edge - chan]], 0))
    middle = back_ref.shape[1] // 2
    return jnp.concatenate(
        [
            dot_wide(back_ref[0, :middle], back_ref[1, :middle], high, low),
            dot_wide(back_ref[0, middle:], back_ref[1, middle:], high, low),
        ],
        0,
    )


def filter_kernel(
    rows, chan, embed_ref, first_bias_ref, freq_ref, inner_ref, second_bias_ref, weight_ref, decay_ref, conv_taps_ref,
    skip_ref, band_ref, into_ref, pair_ref, twiddle_ref, spec_re_ref, spec_im_ref, param_ref,
    first_table, second_table, taps_ref, energy_ref, near_ref, far_ref, embed, first_w, second_w, last_w,
    into, pair, arrivals,
):
    fetches = [
        pltpu.make_async_copy(source, target, arrivals.at[k])
        for k, (source, target) in enumerate(((into_ref, into), (pair_ref, pair)))
    ]
    for fetch in fetches:
        fetch.start()
    block = taps_ref.shape[2]
    hidden = freq_ref.shape[1]
    seq_len = rows * block
    orders = skip_ref.shape[0]
    parts = 2 * orders * chan
    width = embed.shape[0]
    columns = skip_ref.shape[1]
    freq = freq_ref[...] * (0.5 / math.pi)
    second_bias = second_bias_ref[...] * freq - 0.25
    count = embed_ref.shape[0]
    embed[...] = jnp.zeros_like(embed)
    embed[:count, :] = embed_ref[...] * freq
    embed[count : count + 1, :] = first_bias_ref[...] * freq - 0.25
    w_one, w_two = halves(embed[...])
    first_w[...] = jnp.concatenate([w_one, w_one, w_two, jnp.zeros_like(w_two)], 0)
    v_one, v_two = halves(inner_ref[...] * freq)
    second_w[:, :hidden] = jnp.concatenate([v_one, v_one], 0)
    second_w[:, hidden:] = jnp.concatenate([v_two, v_two], 0)
    place = lax.broadcasted_iota(jnp.int32, (chan, columns), 1) - lax.axis_index("row") * chan
    chosen = (place == lax.broadcasted_iota(jnp.int32, (chan, columns), 0)).astype(F32).astype(BF16)

    def choose(table):
        return lax.dot_general(chosen, table, (((1,), (1,)), ((), ())), preferred_element_type=F32)

    def choose_exactly(table):
        return sum(choose(part) for part in thirds(table))

    for k in range(2 * orders):
        u_one, u_two = (
            choose(part).astype(BF16) for part in halves(weight_ref[k // 2, k % 2])
        )
        last_w[k * chan : (k + 1) * chan, :] = jnp.concatenate([u_one, u_one], 1)
        last_w[parts + k * chan : parts + (k + 1) * chan, :] = jnp.concatenate([u_two, jnp.zeros_like(u_two)], 1)
    decay = []
    for order in range(orders):
        here = choose_exactly(decay_ref[order])
        decay += [here[:, 0:1], here[:, 1:2]]
    decay = jnp.concatenate(decay, 0)
    for k in range(conv_taps_ref.shape[0]):
        param_ref[k, :, 0:3] = choose(conv_taps_ref[k])
    param_ref[conv_taps_ref.shape[0], :, 0:orders] = choose_exactly(skip_ref[...])
    band = band_ref[0:1]
    shift = band_ref[1:2]
    line = band_ref[2:3]
    lag = lax.broadcasted_iota(jnp.int32, (block, 2 * width), 0).astype(F32)
    turns = lag * band * (1.0 / seq_len)
    first_table[...] = jnp.where(line > 0, 1.0, cos_turns(turns + shift))
    second_table[...] = jnp.where(line > 0, lag * (1.0 / seq_len), cos_turns(turns + (shift + 0.25)))
    start = lax.broadcasted_iota(jnp.int32, (rows, 2 * width), 0).astype(F32)
    turns = start * band * (1.0 / rows)
    near_ref[...] = jnp.where(line > 0, start * (1.0 / rows), cos_turns(turns))
    far_ref[...] = jnp.where(line > 0, 1.0, cos_turns(turns - 0.25))
    energy_ref[...] = jnp.zeros_like(energy_ref)
    lanes = lax.broadcasted_iota(jnp.int32, (1, block), 1)
    left = lax.broadcasted_iota(jnp.int32, (1, 2 * width), 1) < width
    is_back = (lax.broadcasted_iota(jnp.int32, (parts, 1), 0) // chan) % 2 == 1

    def lags(row):
        feature = first_table[...] * near_ref[pl.ds(row, 1), :] + second_table[...] * far_ref[pl.ds(row, 1), :]
        x_one, x_two = halves(feature)
        layer_one = cos_turns(dot(jnp.concatenate([jnp.where(left, x_one, x_two), x_one], 1), first_w[...]))
        y_one, y_two = halves(layer_one)
        both = dot(jnp.concatenate([y_one, y_two], 1), second_w[...])
        layer_two = cos_turns(both[:, :hidden] + both[:, hidden:] + second_bias)
        z_one, z_two = halves(layer_two)
        both = lax.dot_general(
            last_w[...], jnp.concatenate([z_one, z_two], 1), (((1,), (1,)), ((), ())), preferred_element_type=F32
        )
        raw = both[:parts] + both[parts:]
        at = lanes + row * block
        taps = raw * jnp.exp(decay * (at.astype(F32) * (-1.0 / seq_len)))
        return jnp.where(is_back & (at == 0), 0.0, taps)

    @pl.loop(0, rows // UNROLL)
    def _(step):
        found = [lags(UNROLL * step + k) for k in range(UNROLL)]
        energy_ref[...] += sum(taps * taps for taps in found)
        for k in range(UNROLL):
            place = pl.multiple_of((UNROLL * step + k) * chan, chan)
            for order in range(parts // (2 * chan)):
                base = order * 2 * chan
                ahead = found[k][base : base + chan]
                behind = found[k][base + chan : base + 2 * chan]
                taps_ref[2 * order, pl.ds(place, chan), :] = ahead + behind
                taps_ref[2 * order + 1, pl.ds(place, chan), :] = ahead - behind

    for fetch in fetches:
        fetch.wait()
    total = jnp.sum(energy_ref[...], axis=1, keepdims=True)
    cos_part, sin_part = spread(twiddle_ref, 0, chan), spread(twiddle_ref, 1, chan)
    for order in range(parts // (2 * chan)):
        base = order * 2 * chan
        scale = lax.rsqrt(total[base : base + chan] + total[base + chan : base + 2 * chan] + ENERGY_FLOOR)
        scale = jnp.broadcast_to(scale[None], (rows + 1, chan, block)).reshape(-1, block)
        even_re, even_im = first_stage(taps_ref[2 * order], into, chan)
        odd_re, odd_im = first_stage(taps_ref[2 * order + 1], into, chan)
        spec_re_ref[order] = scale * pair_product(
            even_re * cos_part + even_im * sin_part, even_im * cos_part - even_re * sin_part, pair
        )
        spec_im_ref[order] = scale * pair_product(
            odd_im * cos_part - odd_re * sin_part, -(odd_re * cos_part + odd_im * sin_part), pair
        )


def short(signal, taps, rows, chan):
    block = signal.shape[1]
    lanes = lax.broadcasted_iota(jnp.int32, signal.shape, 1)
    line = lax.broadcasted_iota(jnp.int32, signal.shape, 0)
    size = signal.shape[0]
    before = pltpu.roll(signal, 1, 1)
    crossed = jnp.where(line < chan, 0.0, pltpu.roll(before, chan, 0))
    before = jnp.where(lanes == 0, crossed, before)
    after = pltpu.roll(signal, block - 1, 1)
    crossed = jnp.where(line >= size - chan, 0.0, pltpu.roll(after, size - chan, 0))
    after = jnp.where(lanes == block - 1, crossed, after)

    def tap(k):
        column = taps[:, k : k + 1]
        return jnp.broadcast_to(column[None], (rows, chan, block)).reshape(size, block)

    return before * tap(0) + signal * tap(1) + after * tap(2)


def conv_kernel(
    rows, chan, orders, arrived_ref, param_ref, spec_re_ref, spec_im_ref, into_ref, back_ref, pair_ref,
    twiddle_ref, out_ref,
):
    block = arrived_ref.shape[2]
    size = rows * chan

    def signal(k):
        return arrived_ref[:, k * chan : (k + 1) * chan, :].astype(F32).reshape(size, block)

    cos_part, sin_part = spread(twiddle_ref, 0, chan), spread(twiddle_ref, 1, chan)
    current = short(signal(0), param_ref[orders], rows, chan)
    for order in range(orders):
        data_re, data_im = forward(current, into_ref, pair_ref, cos_part, sin_part, chan)
        spec_re, spec_im = spec_re_ref[order], spec_im_ref[order]
        long_part = backward(
            data_re * spec_re - data_im * spec_im,
            data_re * spec_im + data_im * spec_re,
            back_ref, pair_ref, cos_part, sin_part, chan,
        )
        column = param_ref[orders + 1, :, order : order + 1]
        skip = jnp.broadcast_to(column[None], (rows, chan, block)).reshape(size, block)
        current = long_part + skip * current
        if order < orders - 1:
            current = current * short(signal(order + 1), param_ref[order], rows, chan)
    out_ref[...] = current.astype(BF16).reshape(rows, chan, block)


def turn_kernel(first_ref, second_ref, out_ref):
    rows = out_ref.shape[0]
    chan = out_ref.shape[1] // 2
    for k, ref in enumerate((first_ref, second_ref)):
        turned = jnp.transpose(ref[...].astype(F32)).astype(BF16)
        out_ref[:, k * chan : (k + 1) * chan, :] = turned.reshape(rows, chan, -1)


def gate_kernel(mixed_ref, gate_ref, halo_ref, taps_ref, out_ref):
    gate = gate_ref[...].astype(F32)
    block = gate.shape[0]
    line = lax.broadcasted_iota(jnp.int32, gate.shape, 0)
    halo = halo_ref[...].astype(F32)
    taps = taps_ref[...].astype(F32)
    before = jnp.where(line == 0, halo[0:1], pltpu.roll(gate, 1, 0))
    after = jnp.where(line == block - 1, halo[1:2], pltpu.roll(gate, block - 1, 0))
    factor = before * taps[0:1] + gate * taps[1:2] + after * taps[2:3]
    gated = (jnp.transpose(mixed_ref[...].astype(F32)) * factor).astype(BF16)
    for peer in range(out_ref.shape[0]):
        out_ref[peer] = gated


def call(kernel, out_shape, scratch=(), flops=0, grant=None, placed=None):
    specs = {} if placed is None else {"in_specs": [pl.BlockSpec(memory_space=space) for space in placed]}
    return pl.pallas_call(
        kernel,
        out_shape=out_shape,
        **specs,
        scratch_shapes=scratch,
        cost_estimate=pl.CostEstimate(flops=flops, bytes_accessed=0, transcendentals=0),
        compiler_params=pltpu.CompilerParams(vmem_limit_bytes=grant),
    )


def per_device(
    gate_one, gate_two, values, conv_taps, embed_weight, embed_bias, sine_freq, inner_weight, inner_bias,
    filter_weight, decay_rate, skip_gain, out_weight,
):
    rows = lax.axis_size("row")
    block, columns = gate_one.shape
    orders = skip_gain.shape[0]
    chan = columns // rows
    hidden = sine_freq.shape[0]
    features = embed_weight.shape[0]
    peers = lax.axis_size("col")
    bands = (features - 1) // 2
    into, back, pair, twiddle = tables(rows, chan, block)

    turned = call(turn_kernel, jax.ShapeDtypeStruct((rows, 2 * chan, block), BF16))(values, gate_one)
    arrived = lax.all_to_all(turned, "row", 0, 0, tiled=True)

    down = [(k, k + 1) for k in range(rows - 1)]
    up = [(k + 1, k) for k in range(rows - 1)]
    halo = [lax.ppermute(gate_two[-1:], "row", down), lax.ppermute(gate_two[:1], "row", up)]
    halo = jnp.concatenate(halo, 0)

    width = 64
    steps = np.linspace(0.0001, bands - 1, bands).astype(np.float32)
    band = np.zeros((3, width), np.float32)
    band[0, 1:features] = np.concatenate([steps, steps])
    band[1, 1 + bands : features] = 0.25
    band[2, 0] = 1
    band[:, features:] = 0
    band = np.concatenate([band, band], 1)

    edge = (rows + 1) * chan
    parts = 2 * orders * chan
    spec_shape = jax.ShapeDtypeStruct((orders, edge, block), F32)
    vmem, anywhere = pltpu.VMEM, pl.ANY
    spec_re, spec_im, param = call(
        functools.partial(filter_kernel, rows, chan),
        (spec_shape, spec_shape, jax.ShapeDtypeStruct((conv_taps.shape[0] + 1, chan, 4), F32)),
        (
            pltpu.VMEM((block, 2 * width), F32),
            pltpu.VMEM((block, 2 * width), F32),
            pltpu.VMEM((parts // chan, rows * chan, block), F32),
            pltpu.VMEM((parts, block), F32),
            pltpu.VMEM((rows, 2 * width), F32),
            pltpu.VMEM((rows, 2 * width), F32),
            pltpu.VMEM((width, hidden), F32),
            pltpu.VMEM((4 * width, hidden), BF16),
            pltpu.VMEM((2 * hidden, 2 * hidden), BF16),
            pltpu.VMEM((2 * parts, 2 * hidden), BF16),
            pltpu.VMEM(into.shape, BF16),
            pltpu.VMEM(pair.shape, BF16),
            pltpu.SemaphoreType.DMA((2,)),
        ),
        flops=12_000_000_000,
        placed=[vmem] * 10 + [anywhere] * 2 + [vmem],
    )(
        embed_weight, embed_bias[None], sine_freq[None], inner_weight, inner_bias[None],
        jnp.transpose(filter_weight, (1, 2, 0, 3)), decay_rate, conv_taps, skip_gain, band, into, pair, twiddle,
    )
    mixed = call(
        functools.partial(conv_kernel, rows, chan, orders),
        jax.ShapeDtypeStruct((rows, chan, block), BF16),
        flops=5_000_000_000,
    )(arrived, param, spec_re, spec_im, into, back, pair, twiddle)
    mixed = lax.all_to_all(mixed, "row", 0, 0, tiled=True).reshape(columns, block)
    gated = call(gate_kernel, jax.ShapeDtypeStruct((peers, block, columns), BF16), grant=12 << 20)(
        mixed, gate_two, halo, conv_taps[1]
    )
    return finish(gated, out_weight)


def finish(gated, out_weight):
    peers, block, columns = gated.shape
    everyone = lax.all_to_all(gated, "col", 0, 0, tiled=True)
    weight = out_weight.reshape(peers, columns, -1)
    return jnp.einsum("crk,ckn->rn", everyone, weight, preferred_element_type=F32).astype(BF16)


def solution(mesh):
    spread_rows = ("grp", "row")
    in_specs = (
        P(spread_rows, "col"),
        P(spread_rows, "col"),
        P(spread_rows, "col"),
        P(None, None, "col"),
        P(),
        P(),
        P(),
        P(),
        P(),
        P(None, None, None, "col"),
        P(None, None, "col"),
        P(None, "col"),
        P(None, "col"),
    )
    return jax.shard_map(
        per_device, mesh=mesh, in_specs=in_specs, out_specs=P(spread_rows, "col"), check_vma=False
    )
```

```python
import functools
import math

import jax
import jax.numpy as jnp
import numpy as np
from jax import lax
from jax.experimental import pallas as pl
from jax.experimental.pallas import tpu as pltpu
from jax.sharding import PartitionSpec as P

ENERGY_FLOOR = 1.0
UNROLL = 8
F32 = jnp.float32
BF16 = jnp.bfloat16


def halves(value):
    high = value.astype(BF16)
    return high, (value - high.astype(F32)).astype(BF16)


def thirds(value):
    high = value.astype(BF16)
    rest = value - high.astype(F32)
    middle = rest.astype(BF16)
    return high, middle, (rest - middle.astype(F32)).astype(BF16)


def dot(left, right):
    return jnp.dot(left, right, preferred_element_type=F32)


def dot_wide(left_high, left_low, right_high, right_low):
    return dot(
        jnp.concatenate([left_high, left_low, left_high], 1),
        jnp.concatenate([right_high, right_high, right_low], 0),
    )


def cos_turns(turns):
    near = turns - jnp.round(turns)
    quarter = jnp.abs(near) - 0.25
    square = quarter * quarter
    total = jnp.full_like(square, SINE[-1])
    for factor in SINE[-2::-1]:
        total = total * square + factor
    return total * quarter


def fit_sine():
    nodes = 0.25 * np.cos(np.pi * (np.arange(64) + 0.5) / 128)
    powers = np.stack([nodes ** (2 * i + 1) for i in range(4)], 1)
    return [float(v) for v in np.linalg.lstsq(powers, -np.sin(2 * np.pi * nodes), rcond=None)[0]]


SINE = fit_sine()


def split_constant(table):
    high = table.astype(np.float32).astype(jnp.bfloat16)
    return np.stack([high, (table - high.astype(np.float64)).astype(np.float32).astype(jnp.bfloat16)])


@functools.lru_cache
def tables(rows, chan, block):
    waves = 2 * rows
    half = np.arange(rows + 1)
    phase = 2 * np.pi * (half[:, None] * np.arange(rows)[None] % waves) / waves
    weight = np.where((half == 0) | (half == rows), 1.0, 2.0)[:, None] / (waves * block)
    eye = np.eye(chan)
    into = np.concatenate([np.kron(np.cos(phase), eye), np.kron(-np.sin(phase[1:-1]), eye)])
    back = np.concatenate(
        [np.kron(weight * np.cos(phase), eye), np.kron(-(weight * np.sin(phase))[1:-1], eye)]
    ).T
    inner = 2 * np.pi * (np.arange(block)[:, None] * np.arange(block)[None] % block) / block
    pair = np.concatenate([np.cos(inner), np.sin(inner)], 0)
    turn = 2 * np.pi * half[:, None] * np.arange(block)[None] / (waves * block)
    twiddle = np.stack([np.cos(turn), np.sin(turn)]).astype(np.float32)
    return split_constant(into), split_constant(back), split_constant(pair), twiddle


def spread(twiddle_ref, part, chan):
    value = twiddle_ref[part]
    return jnp.broadcast_to(value[:, None, :], (value.shape[0], chan, value.shape[1])).reshape(-1, value.shape[1])


def first_stage(field, into_ref, chan):
    edge = field.shape[0] + chan
    high, low = halves(field)
    part_re = dot_wide(into_ref[0, :edge], into_ref[1, :edge], high, low)
    part_im = dot_wide(into_ref[0, edge:], into_ref[1, edge:], high, low)
    zero = jnp.zeros((chan, field.shape[1]), F32)
    return part_re, jnp.concatenate([zero, part_im, zero], 0)


def pair_product(first, second, pair_ref):
    first_high, first_low = halves(first)
    second_high, second_low = halves(second)
    return dot_wide(
        jnp.concatenate([first_high, second_high], 1),
        jnp.concatenate([first_low, second_low], 1),
        pair_ref[0],
        pair_ref[1],
    )


def forward(field, into_ref, pair_ref, cos_part, sin_part, chan):
    part_re, part_im = first_stage(field, into_ref, chan)
    turned_re = part_re * cos_part + part_im * sin_part
    turned_im = part_im * cos_part - part_re * sin_part
    return pair_product(turned_re, turned_im, pair_ref), pair_product(turned_im, -turned_re, pair_ref)


def backward(part_re, part_im, back_ref, pair_ref, cos_part, sin_part, chan):
    edge = part_re.shape[0]
    wave_re = pair_product(part_re, -part_im, pair_ref)
    wave_im = pair_product(part_im, part_re, pair_ref)
    turned_re = wave_re * cos_part - wave_im * sin_part
    turned_im = wave_re * sin_part + wave_im * cos_part
    high, low = halves(jnp.concatenate([turned_re, turned_im[chan : edge - chan]], 0))
    middle = back_ref.shape[1] // 2
    return jnp.concatenate(
        [
            dot_wide(back_ref[0, :middle], back_ref[1, :middle], high, low),
            dot_wide(back_ref[0, middle:], back_ref[1, middle:], high, low),
        ],
        0,
    )


def filter_kernel(
    rows, chan, embed_ref, first_bias_ref, freq_ref, inner_ref, second_bias_ref, weight_ref, decay_ref, conv_taps_ref,
    skip_ref, band_ref, into_ref, pair_ref, twiddle_ref, spec_re_ref, spec_im_ref, param_ref,
    first_table, second_table, taps_ref, energy_ref, near_ref, far_ref, embed, first_w, second_w, last_w,
    into, pair, arrivals,
):
    fetches = [
        pltpu.make_async_copy(source, target, arrivals.at[k])
        for k, (source, target) in enumerate(((into_ref, into), (pair_ref, pair)))
    ]
    for fetch in fetches:
        fetch.start()
    block = taps_ref.shape[2]
    hidden = freq_ref.shape[1]
    seq_len = rows * block
    orders = skip_ref.shape[0]
    parts = 2 * orders * chan
    width = embed.shape[0]
    columns = skip_ref.shape[1]
    freq = freq_ref[...] * (0.5 / math.pi)
    second_bias = second_bias_ref[...] * freq - 0.25
    count = embed_ref.shape[0]
    embed[...] = jnp.zeros_like(embed)
    embed[:count, :] = embed_ref[...] * freq
    embed[count : count + 1, :] = first_bias_ref[...] * freq - 0.25
    w_one, w_two = halves(embed[...])
    first_w[...] = jnp.concatenate([w_one, w_one, w_two, jnp.zeros_like(w_two)], 0)
    v_one, v_two = halves(inner_ref[...] * freq)
    second_w[:, :hidden] = jnp.concatenate([v_one, v_one], 0)
    second_w[:, hidden:] = jnp.concatenate([v_two, v_two], 0)
    place = lax.broadcasted_iota(jnp.int32, (chan, columns), 1) - lax.axis_index("row") * chan
    chosen = (place == lax.broadcasted_iota(jnp.int32, (chan, columns), 0)).astype(F32).astype(BF16)

    def choose(table):
        return lax.dot_general(chosen, table, (((1,), (1,)), ((), ())), preferred_element_type=F32)

    def choose_exactly(table):
        return sum(choose(part) for part in thirds(table))

    for k in range(2 * orders):
        u_one, u_two = (
            choose(part).astype(BF16) for part in halves(weight_ref[k // 2, k % 2])
        )
        last_w[k * chan : (k + 1) * chan, :] = jnp.concatenate([u_one, u_one], 1)
        last_w[parts + k * chan : parts + (k + 1) * chan, :] = jnp.concatenate([u_two, jnp.zeros_like(u_two)], 1)
    decay = []
    for order in range(orders):
        here = choose_exactly(decay_ref[order])
        decay += [here[:, 0:1], here[:, 1:2]]
    decay = jnp.concatenate(decay, 0)
    for k in range(conv_taps_ref.shape[0]):
        param_ref[k, :, 0:3] = choose(conv_taps_ref[k])
    param_ref[conv_taps_ref.shape[0], :, 0:orders] = choose_exactly(skip_ref[...])
    band = band_ref[0:1]
    shift = band_ref[1:2]
    line = band_ref[2:3]
    lag = lax.broadcasted_iota(jnp.int32, (block, 2 * width), 0).astype(F32)
    turns = lag * band * (1.0 / seq_len)
    first_table[...] = jnp.where(line > 0, 1.0, cos_turns(turns + shift))
    second_table[...] = jnp.where(line > 0, lag * (1.0 / seq_len), cos_turns(turns + (shift + 0.25)))
    start = lax.broadcasted_iota(jnp.int32, (rows, 2 * width), 0).astype(F32)
    turns = start * band * (1.0 / rows)
    near_ref[...] = jnp.where(line > 0, start * (1.0 / rows), cos_turns(turns))
    far_ref[...] = jnp.where(line > 0, 1.0, cos_turns(turns - 0.25))
    energy_ref[...] = jnp.zeros_like(energy_ref)
    lanes = lax.broadcasted_iota(jnp.int32, (1, block), 1)
    left = lax.broadcasted_iota(jnp.int32, (1, 2 * width), 1) < width
    is_back = (lax.broadcasted_iota(jnp.int32, (parts, 1), 0) // chan) % 2 == 1

    def lags(row):
        feature = first_table[...] * near_ref[pl.ds(row, 1), :] + second_table[...] * far_ref[pl.ds(row, 1), :]
        x_one, x_two = halves(feature)
        layer_one = cos_turns(dot(jnp.concatenate([jnp.where(left, x_one, x_two), x_one], 1), first_w[...]))
        y_one, y_two = halves(layer_one)
        both = dot(jnp.concatenate([y_one, y_two], 1), second_w[...])
        layer_two = cos_turns(both[:, :hidden] + both[:, hidden:] + second_bias)
        z_one, z_two = halves(layer_two)
        both = lax.dot_general(
            last_w[...], jnp.concatenate([z_one, z_two], 1), (((1,), (1,)), ((), ())), preferred_element_type=F32
        )
        raw = both[:parts] + both[parts:]
        at = lanes + row * block
        taps = raw * jnp.exp(decay * (at.astype(F32) * (-1.0 / seq_len)))
        return jnp.where(is_back & (at == 0), 0.0, taps)

    @pl.loop(0, rows // UNROLL)
    def _(step):
        found = [lags(UNROLL * step + k) for k in range(UNROLL)]
        energy_ref[...] += sum(taps * taps for taps in found)
        for k in range(UNROLL):
            place = pl.multiple_of((UNROLL * step + k) * chan, chan)
            for order in range(parts // (2 * chan)):
                base = order * 2 * chan
                ahead = found[k][base : base + chan]
                behind = found[k][base + chan : base + 2 * chan]
                taps_ref[2 * order, pl.ds(place, chan), :] = ahead + behind
                taps_ref[2 * order + 1, pl.ds(place, chan), :] = ahead - behind

    for fetch in fetches:
        fetch.wait()
    total = jnp.sum(energy_ref[...], axis=1, keepdims=True)
    cos_part, sin_part = spread(twiddle_ref, 0, chan), spread(twiddle_ref, 1, chan)
    for order in range(parts // (2 * chan)):
        base = order * 2 * chan
        scale = lax.rsqrt(total[base : base + chan] + total[base + chan : base + 2 * chan] + ENERGY_FLOOR)
        scale = jnp.broadcast_to(scale[None], (rows + 1, chan, block)).reshape(-1, block)
        even_re, even_im = first_stage(taps_ref[2 * order], into, chan)
        odd_re, odd_im = first_stage(taps_ref[2 * order + 1], into, chan)
        spec_re_ref[order] = scale * pair_product(
            even_re * cos_part + even_im * sin_part, even_im * cos_part - even_re * sin_part, pair
        )
        spec_im_ref[order] = scale * pair_product(
            odd_im * cos_part - odd_re * sin_part, -(odd_re * cos_part + odd_im * sin_part), pair
        )


def short(signal, taps, rows, chan):
    block = signal.shape[1]
    lanes = lax.broadcasted_iota(jnp.int32, signal.shape, 1)
    line = lax.broadcasted_iota(jnp.int32, signal.shape, 0)
    size = signal.shape[0]
    before = pltpu.roll(signal, 1, 1)
    crossed = jnp.where(line < chan, 0.0, pltpu.roll(before, chan, 0))
    before = jnp.where(lanes == 0, crossed, before)
    after = pltpu.roll(signal, block - 1, 1)
    crossed = jnp.where(line >= size - chan, 0.0, pltpu.roll(after, size - chan, 0))
    after = jnp.where(lanes == block - 1, crossed, after)

    def tap(k):
        column = taps[:, k : k + 1]
        return jnp.broadcast_to(column[None], (rows, chan, block)).reshape(size, block)

    return before * tap(0) + signal * tap(1) + after * tap(2)


def conv_kernel(
    rows, chan, orders, arrived_ref, param_ref, spec_re_ref, spec_im_ref, into_ref, back_ref, pair_ref,
    twiddle_ref, out_ref,
):
    block = arrived_ref.shape[2]
    size = rows * chan

    def signal(k):
        return arrived_ref[:, k * chan : (k + 1) * chan, :].astype(F32).reshape(size, block)

    cos_part, sin_part = spread(twiddle_ref, 0, chan), spread(twiddle_ref, 1, chan)
    current = short(signal(0), param_ref[orders], rows, chan)
    for order in range(orders):
        data_re, data_im = forward(current, into_ref, pair_ref, cos_part, sin_part, chan)
        spec_re, spec_im = spec_re_ref[order], spec_im_ref[order]
        long_part = backward(
            data_re * spec_re - data_im * spec_im,
            data_re * spec_im + data_im * spec_re,
            back_ref, pair_ref, cos_part, sin_part, chan,
        )
        column = param_ref[orders + 1, :, order : order + 1]
        skip = jnp.broadcast_to(column[None], (rows, chan, block)).reshape(size, block)
        current = long_part + skip * current
        if order < orders - 1:
            current = current * short(signal(order + 1), param_ref[order], rows, chan)
    out_ref[...] = current.astype(BF16).reshape(rows, chan, block)


def turn_kernel(first_ref, second_ref, out_ref):
    rows = out_ref.shape[0]
    chan = out_ref.shape[1] // 2
    for k, ref in enumerate((first_ref, second_ref)):
        turned = jnp.transpose(ref[...].astype(F32)).astype(BF16)
        out_ref[:, k * chan : (k + 1) * chan, :] = turned.reshape(rows, chan, -1)


def gate_kernel(mixed_ref, gate_ref, halo_ref, taps_ref, out_ref):
    gate = gate_ref[...].astype(F32)
    block = gate.shape[0]
    line = lax.broadcasted_iota(jnp.int32, gate.shape, 0)
    halo = halo_ref[...].astype(F32)
    taps = taps_ref[...].astype(F32)
    before = jnp.where(line == 0, halo[0:1], pltpu.roll(gate, 1, 0))
    after = jnp.where(line == block - 1, halo[1:2], pltpu.roll(gate, block - 1, 0))
    factor = before * taps[0:1] + gate * taps[1:2] + after * taps[2:3]
    out_ref[...] = (jnp.transpose(mixed_ref[...].astype(F32)) * factor).astype(BF16)


def call(kernel, out_shape, scratch=(), flops=0, grant=None, placed=None):
    specs = {} if placed is None else {"in_specs": [pl.BlockSpec(memory_space=space) for space in placed]}
    return pl.pallas_call(
        kernel,
        out_shape=out_shape,
        **specs,
        scratch_shapes=scratch,
        cost_estimate=pl.CostEstimate(flops=flops, bytes_accessed=0, transcendentals=0),
        compiler_params=pltpu.CompilerParams(vmem_limit_bytes=grant),
    )


def per_device(
    gate_one, gate_two, values, conv_taps, embed_weight, embed_bias, sine_freq, inner_weight, inner_bias,
    filter_weight, decay_rate, skip_gain, out_weight,
):
    rows = lax.axis_size("row")
    block, columns = gate_one.shape
    orders = skip_gain.shape[0]
    chan = columns // rows
    hidden = sine_freq.shape[0]
    features = embed_weight.shape[0]
    bands = (features - 1) // 2
    into, back, pair, twiddle = tables(rows, chan, block)

    turned = call(turn_kernel, jax.ShapeDtypeStruct((rows, 2 * chan, block), BF16))(values, gate_one)
    arrived = lax.all_to_all(turned, "row", 0, 0, tiled=True)

    down = [(k, k + 1) for k in range(rows - 1)]
    up = [(k + 1, k) for k in range(rows - 1)]
    halo = [lax.ppermute(gate_two[-1:], "row", down), lax.ppermute(gate_two[:1], "row", up)]
    halo = jnp.concatenate(halo, 0)

    width = 64
    steps = np.linspace(0.0001, bands - 1, bands).astype(np.float32)
    band = np.zeros((3, width), np.float32)
    band[0, 1:features] = np.concatenate([steps, steps])
    band[1, 1 + bands : features] = 0.25
    band[2, 0] = 1
    band[:, features:] = 0
    band = np.concatenate([band, band], 1)

    edge = (rows + 1) * chan
    parts = 2 * orders * chan
    spec_shape = jax.ShapeDtypeStruct((orders, edge, block), F32)
    vmem, anywhere = pltpu.VMEM, pl.ANY
    spec_re, spec_im, param = call(
        functools.partial(filter_kernel, rows, chan),
        (spec_shape, spec_shape, jax.ShapeDtypeStruct((conv_taps.shape[0] + 1, chan, 4), F32)),
        (
            pltpu.VMEM((block, 2 * width), F32),
            pltpu.VMEM((block, 2 * width), F32),
            pltpu.VMEM((parts // chan, rows * chan, block), F32),
            pltpu.VMEM((parts, block), F32),
            pltpu.VMEM((rows, 2 * width), F32),
            pltpu.VMEM((rows, 2 * width), F32),
            pltpu.VMEM((width, hidden), F32),
            pltpu.VMEM((4 * width, hidden), BF16),
            pltpu.VMEM((2 * hidden, 2 * hidden), BF16),
            pltpu.VMEM((2 * parts, 2 * hidden), BF16),
            pltpu.VMEM(into.shape, BF16),
            pltpu.VMEM(pair.shape, BF16),
            pltpu.SemaphoreType.DMA((2,)),
        ),
        flops=12_000_000_000,
        placed=[vmem] * 10 + [anywhere] * 2 + [vmem],
    )(
        embed_weight, embed_bias[None], sine_freq[None], inner_weight, inner_bias[None],
        jnp.transpose(filter_weight, (1, 2, 0, 3)), decay_rate, conv_taps, skip_gain, band, into, pair, twiddle,
    )
    mixed = call(
        functools.partial(conv_kernel, rows, chan, orders),
        jax.ShapeDtypeStruct((rows, chan, block), BF16),
        flops=5_000_000_000,
    )(arrived, param, spec_re, spec_im, into, back, pair, twiddle)
    mixed = lax.all_to_all(mixed, "row", 0, 0, tiled=True).reshape(columns, block)
    gated = call(gate_kernel, jax.ShapeDtypeStruct((block, columns), BF16), grant=12 << 20)(
        mixed, gate_two, halo, conv_taps[1]
    )
    return finish(gated, out_weight)


def product_kernel(shifts, weight_ref, *refs):
    out_ref = refs[-1]
    peers = weight_ref.shape[0]
    me = lax.axis_index("col")
    half = out_ref.shape[0] // 2
    for part in range(2):
        place = slice(part * half, (part + 1) * half)
        total = None
        for shift, ref in zip(shifts, refs):
            term = dot(ref[place, :], weight_ref[lax.rem(me + (peers - shift), peers)])
            total = term if total is None else total + term
        out_ref[place, :] = total.astype(BF16)


def finish(gated, out_weight):
    peers = lax.axis_size("col")
    columns = gated.shape[1]

    def shifted(block, shift):
        return lax.ppermute(block, "col", [(k, (k + shift) % peers) for k in range(peers)])

    blocks = {0: gated}
    for shift in (2, peers - 2, 1, peers - 1):
        blocks[shift] = shifted(gated, shift)
    blocks[4] = shifted(blocks[2], 2)
    blocks[3] = shifted(blocks[2], 1)
    blocks[peers - 3] = shifted(blocks[peers - 2], peers - 1)
    weight = out_weight.reshape(peers, columns, -1)
    return call(
        functools.partial(product_kernel, tuple(blocks)),
        jax.ShapeDtypeStruct((gated.shape[0], weight.shape[2]), BF16),
        flops=1_000_000_000,
        grant=12 << 20,
    )(weight, *blocks.values())


def solution(mesh):
    spread_rows = ("grp", "row")
    in_specs = (
        P(spread_rows, "col"),
        P(spread_rows, "col"),
        P(spread_rows, "col"),
        P(None, None, "col"),
        P(),
        P(),
        P(),
        P(),
        P(),
        P(None, None, None, "col"),
        P(None, None, "col"),
        P(None, "col"),
        P(None, "col"),
    )
    return jax.shard_map(
        per_device, mesh=mesh, in_specs=in_specs, out_specs=P(spread_rows, "col"), check_vma=False
    )
```

```python
import functools
import math

import jax
import jax.numpy as jnp
import numpy as np
from jax import lax
from jax.experimental import pallas as pl
from jax.experimental.pallas import tpu as pltpu
from jax.sharding import PartitionSpec as P

ENERGY_FLOOR = 1.0
UNROLL = 8
F32 = jnp.float32
BF16 = jnp.bfloat16


def halves(value):
    high = value.astype(BF16)
    return high, (value - high.astype(F32)).astype(BF16)


def thirds(value):
    high = value.astype(BF16)
    rest = value - high.astype(F32)
    middle = rest.astype(BF16)
    return high, middle, (rest - middle.astype(F32)).astype(BF16)


def dot(left, right):
    return jnp.dot(left, right, preferred_element_type=F32)


def dot_wide(left_high, left_low, right_high, right_low):
    return dot(
        jnp.concatenate([left_high, left_low, left_high], 1),
        jnp.concatenate([right_high, right_high, right_low], 0),
    )


def cos_turns(turns):
    near = turns - jnp.round(turns)
    quarter = jnp.abs(near) - 0.25
    square = quarter * quarter
    total = jnp.full_like(square, SINE[-1])
    for factor in SINE[-2::-1]:
        total = total * square + factor
    return total * quarter


def fit_sine():
    nodes = 0.25 * np.cos(np.pi * (np.arange(64) + 0.5) / 128)
    powers = np.stack([nodes ** (2 * i + 1) for i in range(4)], 1)
    return [float(v) for v in np.linalg.lstsq(powers, -np.sin(2 * np.pi * nodes), rcond=None)[0]]


SINE = fit_sine()


def split_constant(table):
    high = table.astype(np.float32).astype(jnp.bfloat16)
    return np.stack([high, (table - high.astype(np.float64)).astype(np.float32).astype(jnp.bfloat16)])


@functools.lru_cache
def tables(rows, chan, block):
    waves = 2 * rows
    half = np.arange(rows + 1)
    phase = 2 * np.pi * (half[:, None] * np.arange(rows)[None] % waves) / waves
    weight = np.where((half == 0) | (half == rows), 1.0, 2.0)[:, None] / (waves * block)
    eye = np.eye(chan)
    into = np.concatenate([np.kron(np.cos(phase), eye), np.kron(-np.sin(phase[1:-1]), eye)])
    back = np.concatenate(
        [np.kron(weight * np.cos(phase), eye), np.kron(-(weight * np.sin(phase))[1:-1], eye)]
    ).T
    inner = 2 * np.pi * (np.arange(block)[:, None] * np.arange(block)[None] % block) / block
    pair = np.concatenate([np.cos(inner), np.sin(inner)], 0)
    turn = 2 * np.pi * half[:, None] * np.arange(block)[None] / (waves * block)
    twiddle = np.stack([np.cos(turn), np.sin(turn)]).astype(np.float32)
    return split_constant(into), split_constant(back), split_constant(pair), twiddle


def spread(twiddle_ref, part, chan):
    value = twiddle_ref[part]
    return jnp.broadcast_to(value[:, None, :], (value.shape[0], chan, value.shape[1])).reshape(-1, value.shape[1])


def first_stage(field, into_ref, chan):
    edge = field.shape[0] + chan
    high, low = halves(field)
    part_re = dot_wide(into_ref[0, :edge], into_ref[1, :edge], high, low)
    part_im = dot_wide(into_ref[0, edge:], into_ref[1, edge:], high, low)
    zero = jnp.zeros((chan, field.shape[1]), F32)
    return part_re, jnp.concatenate([zero, part_im, zero], 0)


def pair_product(first, second, pair_ref):
    first_high, first_low = halves(first)
    second_high, second_low = halves(second)
    return dot_wide(
        jnp.concatenate([first_high, second_high], 1),
        jnp.concatenate([first_low, second_low], 1),
        pair_ref[0],
        pair_ref[1],
    )


def forward(field, into_ref, pair_ref, cos_part, sin_part, chan):
    part_re, part_im = first_stage(field, into_ref, chan)
    turned_re = part_re * cos_part + part_im * sin_part
    turned_im = part_im * cos_part - part_re * sin_part
    return pair_product(turned_re, turned_im, pair_ref), pair_product(turned_im, -turned_re, pair_ref)


def backward(part_re, part_im, back_ref, pair_ref, cos_part, sin_part, chan):
    edge = part_re.shape[0]
    wave_re = pair_product(part_re, -part_im, pair_ref)
    wave_im = pair_product(part_im, part_re, pair_ref)
    turned_re = wave_re * cos_part - wave_im * sin_part
    turned_im = wave_re * sin_part + wave_im * cos_part
    high, low = halves(jnp.concatenate([turned_re, turned_im[chan : edge - chan]], 0))
    middle = back_ref.shape[1] // 2
    return jnp.concatenate(
        [
            dot_wide(back_ref[0, :middle], back_ref[1, :middle], high, low),
            dot_wide(back_ref[0, middle:], back_ref[1, middle:], high, low),
        ],
        0,
    )


def filter_kernel(
    rows, chan, embed_ref, first_bias_ref, freq_ref, inner_ref, second_bias_ref, weight_ref, decay_ref, conv_taps_ref,
    skip_ref, band_ref, into_ref, pair_ref, twiddle_ref, spec_re_ref, spec_im_ref, param_ref,
    first_table, second_table, taps_ref, energy_ref, near_ref, far_ref, embed, first_w, second_w, last_w,
    into, pair, arrivals,
):
    fetches = [
        pltpu.make_async_copy(source, target, arrivals.at[k])
        for k, (source, target) in enumerate(((into_ref, into), (pair_ref, pair)))
    ]
    for fetch in fetches:
        fetch.start()
    block = taps_ref.shape[2]
    hidden = freq_ref.shape[1]
    seq_len = rows * block
    orders = skip_ref.shape[0]
    parts = 2 * orders * chan
    width = embed.shape[0]
    columns = skip_ref.shape[1]
    freq = freq_ref[...] * (0.5 / math.pi)
    second_bias = second_bias_ref[...] * freq - 0.25
    count = embed_ref.shape[0]
    embed[...] = jnp.zeros_like(embed)
    embed[:count, :] = embed_ref[...] * freq
    embed[count : count + 1, :] = first_bias_ref[...] * freq - 0.25
    w_one, w_two = halves(embed[...])
    first_w[...] = jnp.concatenate([w_one, w_one, w_two, jnp.zeros_like(w_two)], 0)
    v_one, v_two = halves(inner_ref[...] * freq)
    second_w[:, :hidden] = jnp.concatenate([v_one, v_one], 0)
    second_w[:, hidden:] = jnp.concatenate([v_two, v_two], 0)
    place = lax.broadcasted_iota(jnp.int32, (chan, columns), 1) - lax.axis_index("row") * chan
    chosen = (place == lax.broadcasted_iota(jnp.int32, (chan, columns), 0)).astype(F32).astype(BF16)

    def choose(table):
        return lax.dot_general(chosen, table, (((1,), (1,)), ((), ())), preferred_element_type=F32)

    def choose_exactly(table):
        return sum(choose(part) for part in thirds(table))

    for k in range(2 * orders):
        u_one, u_two = (
            choose(part).astype(BF16) for part in halves(weight_ref[k // 2, k % 2])
        )
        last_w[k * chan : (k + 1) * chan, :] = jnp.concatenate([u_one, u_one], 1)
        last_w[parts + k * chan : parts + (k + 1) * chan, :] = jnp.concatenate([u_two, jnp.zeros_like(u_two)], 1)
    decay = []
    for order in range(orders):
        here = choose_exactly(decay_ref[order])
        decay += [here[:, 0:1], here[:, 1:2]]
    decay = jnp.concatenate(decay, 0)
    for k in range(conv_taps_ref.shape[0]):
        param_ref[k, :, 0:3] = choose(conv_taps_ref[k])
    param_ref[conv_taps_ref.shape[0], :, 0:orders] = choose_exactly(skip_ref[...])
    band = band_ref[0:1]
    shift = band_ref[1:2]
    line = band_ref[2:3]
    lag = lax.broadcasted_iota(jnp.int32, (block, 2 * width), 0).astype(F32)
    turns = lag * band * (1.0 / seq_len)
    first_table[...] = jnp.where(line > 0, 1.0, cos_turns(turns + shift))
    second_table[...] = jnp.where(line > 0, lag * (1.0 / seq_len), cos_turns(turns + (shift + 0.25)))
    start = lax.broadcasted_iota(jnp.int32, (rows, 2 * width), 0).astype(F32)
    turns = start * band * (1.0 / rows)
    near_ref[...] = jnp.where(line > 0, start * (1.0 / rows), cos_turns(turns))
    far_ref[...] = jnp.where(line > 0, 1.0, cos_turns(turns - 0.25))
    energy_ref[...] = jnp.zeros_like(energy_ref)
    lanes = lax.broadcasted_iota(jnp.int32, (1, block), 1)
    left = lax.broadcasted_iota(jnp.int32, (1, 2 * width), 1) < width
    is_back = (lax.broadcasted_iota(jnp.int32, (parts, 1), 0) // chan) % 2 == 1

    def lags(row):
        feature = first_table[...] * near_ref[pl.ds(row, 1), :] + second_table[...] * far_ref[pl.ds(row, 1), :]
        x_one, x_two = halves(feature)
        layer_one = cos_turns(dot(jnp.concatenate([jnp.where(left, x_one, x_two), x_one], 1), first_w[...]))
        y_one, y_two = halves(layer_one)
        both = dot(jnp.concatenate([y_one, y_two], 1), second_w[...])
        layer_two = cos_turns(both[:, :hidden] + both[:, hidden:] + second_bias)
        z_one, z_two = halves(layer_two)
        both = lax.dot_general(
            last_w[...], jnp.concatenate([z_one, z_two], 1), (((1,), (1,)), ((), ())), preferred_element_type=F32
        )
        raw = both[:parts] + both[parts:]
        at = lanes + row * block
        taps = raw * jnp.exp(decay * (at.astype(F32) * (-1.0 / seq_len)))
        return jnp.where(is_back & (at == 0), 0.0, taps)

    @pl.loop(0, rows // UNROLL)
    def _(step):
        found = [lags(UNROLL * step + k) for k in range(UNROLL)]
        energy_ref[...] += sum(taps * taps for taps in found)
        for k in range(UNROLL):
            place = pl.multiple_of((UNROLL * step + k) * chan, chan)
            for order in range(parts // (2 * chan)):
                base = order * 2 * chan
                ahead = found[k][base : base + chan]
                behind = found[k][base + chan : base + 2 * chan]
                taps_ref[2 * order, pl.ds(place, chan), :] = ahead + behind
                taps_ref[2 * order + 1, pl.ds(place, chan), :] = ahead - behind

    for fetch in fetches:
        fetch.wait()
    total = jnp.sum(energy_ref[...], axis=1, keepdims=True)
    cos_part, sin_part = spread(twiddle_ref, 0, chan), spread(twiddle_ref, 1, chan)
    for order in range(parts // (2 * chan)):
        base = order * 2 * chan
        scale = lax.rsqrt(total[base : base + chan] + total[base + chan : base + 2 * chan] + ENERGY_FLOOR)
        scale = jnp.broadcast_to(scale[None], (rows + 1, chan, block)).reshape(-1, block)
        even_re, even_im = first_stage(taps_ref[2 * order], into, chan)
        odd_re, odd_im = first_stage(taps_ref[2 * order + 1], into, chan)
        spec_re_ref[order] = scale * pair_product(
            even_re * cos_part + even_im * sin_part, even_im * cos_part - even_re * sin_part, pair
        )
        spec_im_ref[order] = scale * pair_product(
            odd_im * cos_part - odd_re * sin_part, -(odd_re * cos_part + odd_im * sin_part), pair
        )


def short(signal, taps, rows, chan):
    block = signal.shape[1]
    lanes = lax.broadcasted_iota(jnp.int32, signal.shape, 1)
    line = lax.broadcasted_iota(jnp.int32, signal.shape, 0)
    size = signal.shape[0]
    before = pltpu.roll(signal, 1, 1)
    crossed = jnp.where(line < chan, 0.0, pltpu.roll(before, chan, 0))
    before = jnp.where(lanes == 0, crossed, before)
    after = pltpu.roll(signal, block - 1, 1)
    crossed = jnp.where(line >= size - chan, 0.0, pltpu.roll(after, size - chan, 0))
    after = jnp.where(lanes == block - 1, crossed, after)

    def tap(k):
        column = taps[:, k : k + 1]
        return jnp.broadcast_to(column[None], (rows, chan, block)).reshape(size, block)

    return before * tap(0) + signal * tap(1) + after * tap(2)


def conv_kernel(
    rows, chan, orders, arrived_ref, param_ref, spec_re_ref, spec_im_ref, into_ref, back_ref, pair_ref,
    twiddle_ref, out_ref,
):
    block = arrived_ref.shape[2]
    size = rows * chan

    def signal(k):
        return arrived_ref[:, k * chan : (k + 1) * chan, :].astype(F32).reshape(size, block)

    cos_part, sin_part = spread(twiddle_ref, 0, chan), spread(twiddle_ref, 1, chan)
    current = short(signal(0), param_ref[orders], rows, chan)
    for order in range(orders):
        data_re, data_im = forward(current, into_ref, pair_ref, cos_part, sin_part, chan)
        spec_re, spec_im = spec_re_ref[order], spec_im_ref[order]
        long_part = backward(
            data_re * spec_re - data_im * spec_im,
            data_re * spec_im + data_im * spec_re,
            back_ref, pair_ref, cos_part, sin_part, chan,
        )
        column = param_ref[orders + 1, :, order : order + 1]
        skip = jnp.broadcast_to(column[None], (rows, chan, block)).reshape(size, block)
        current = long_part + skip * current
        if order < orders - 1:
            current = current * short(signal(order + 1), param_ref[order], rows, chan)
    out_ref[...] = current.astype(BF16).reshape(rows, chan, block)


def turn_kernel(first_ref, second_ref, out_ref, first, second, first_out, second_out, arrivals, departures):
    chan = out_ref.shape[1] // 2
    moves = []
    for k, (ref, held, turned) in enumerate(((first_ref, first, first_out), (second_ref, second, second_out))):
        fetch = pltpu.make_async_copy(ref, held, arrivals.at[k])
        fetch.start()
        leave = pltpu.make_async_copy(turned, out_ref.at[:, pl.ds(k * chan, chan), :], departures.at[k])
        moves.append((fetch, held, turned, leave))
    for fetch, held, turned, leave in moves:
        fetch.wait()
        turned[...] = jnp.transpose(held[...].astype(F32)).astype(BF16).reshape(turned.shape)
        leave.start()
    for _, _, _, leave in moves:
        leave.wait()


def gate_kernel(mixed_ref, gate_ref, halo_ref, taps_ref, out_ref):
    gate = gate_ref[...].astype(F32)
    block = gate.shape[0]
    line = lax.broadcasted_iota(jnp.int32, gate.shape, 0)
    halo = halo_ref[...].astype(F32)
    taps = taps_ref[...].astype(F32)
    before = jnp.where(line == 0, halo[0:1], pltpu.roll(gate, 1, 0))
    after = jnp.where(line == block - 1, halo[1:2], pltpu.roll(gate, block - 1, 0))
    factor = before * taps[0:1] + gate * taps[1:2] + after * taps[2:3]
    out_ref[...] = (jnp.transpose(mixed_ref[...].astype(F32)) * factor).astype(BF16)


def call(kernel, out_shape, scratch=(), flops=0, grant=None, placed=None, result=None):
    specs = {} if placed is None else {"in_specs": [pl.BlockSpec(memory_space=space) for space in placed]}
    if result is not None:
        specs["out_specs"] = pl.BlockSpec(memory_space=result)
    return pl.pallas_call(
        kernel,
        out_shape=out_shape,
        **specs,
        scratch_shapes=scratch,
        cost_estimate=pl.CostEstimate(flops=flops, bytes_accessed=0, transcendentals=0),
        compiler_params=pltpu.CompilerParams(vmem_limit_bytes=grant),
    )


def per_device(
    gate_one, gate_two, values, conv_taps, embed_weight, embed_bias, sine_freq, inner_weight, inner_bias,
    filter_weight, decay_rate, skip_gain, out_weight,
):
    rows = lax.axis_size("row")
    block, columns = gate_one.shape
    orders = skip_gain.shape[0]
    chan = columns // rows
    hidden = sine_freq.shape[0]
    features = embed_weight.shape[0]
    bands = (features - 1) // 2
    into, back, pair, twiddle = tables(rows, chan, block)

    vmem, anywhere = pltpu.VMEM, pl.ANY
    turned = call(
        turn_kernel,
        jax.ShapeDtypeStruct((rows, 2 * chan, block), BF16),
        [pltpu.VMEM((block, columns), BF16)] * 2
        + [pltpu.VMEM((rows, chan, block), BF16)] * 2
        + [pltpu.SemaphoreType.DMA((2,))] * 2,
        placed=[anywhere] * 2,
        result=anywhere,
    )(values, gate_one)
    arrived = lax.all_to_all(turned, "row", 0, 0, tiled=True)

    down = [(k, k + 1) for k in range(rows - 1)]
    up = [(k + 1, k) for k in range(rows - 1)]
    halo = [lax.ppermute(gate_two[-1:], "row", down), lax.ppermute(gate_two[:1], "row", up)]
    halo = jnp.concatenate(halo, 0)

    width = 64
    steps = np.linspace(0.0001, bands - 1, bands).astype(np.float32)
    band = np.zeros((3, width), np.float32)
    band[0, 1:features] = np.concatenate([steps, steps])
    band[1, 1 + bands : features] = 0.25
    band[2, 0] = 1
    band[:, features:] = 0
    band = np.concatenate([band, band], 1)

    edge = (rows + 1) * chan
    parts = 2 * orders * chan
    spec_shape = jax.ShapeDtypeStruct((orders, edge, block), F32)
    spec_re, spec_im, param = call(
        functools.partial(filter_kernel, rows, chan),
        (spec_shape, spec_shape, jax.ShapeDtypeStruct((conv_taps.shape[0] + 1, chan, 4), F32)),
        (
            pltpu.VMEM((block, 2 * width), F32),
            pltpu.VMEM((block, 2 * width), F32),
            pltpu.VMEM((parts // chan, rows * chan, block), F32),
            pltpu.VMEM((parts, block), F32),
            pltpu.VMEM((rows, 2 * width), F32),
            pltpu.VMEM((rows, 2 * width), F32),
            pltpu.VMEM((width, hidden), F32),
            pltpu.VMEM((4 * width, hidden), BF16),
            pltpu.VMEM((2 * hidden, 2 * hidden), BF16),
            pltpu.VMEM((2 * parts, 2 * hidden), BF16),
            pltpu.VMEM(into.shape, BF16),
            pltpu.VMEM(pair.shape, BF16),
            pltpu.SemaphoreType.DMA((2,)),
        ),
        flops=12_000_000_000,
        placed=[vmem] * 10 + [anywhere] * 2 + [vmem],
    )(
        embed_weight, embed_bias[None], sine_freq[None], inner_weight, inner_bias[None],
        jnp.transpose(filter_weight, (1, 2, 0, 3)), decay_rate, conv_taps, skip_gain, band, into, pair, twiddle,
    )
    mixed = call(
        functools.partial(conv_kernel, rows, chan, orders),
        jax.ShapeDtypeStruct((rows, chan, block), BF16),
        flops=5_000_000_000,
    )(arrived, param, spec_re, spec_im, into, back, pair, twiddle)
    mixed = lax.all_to_all(mixed, "row", 0, 0, tiled=True).reshape(columns, block)
    gated = call(gate_kernel, jax.ShapeDtypeStruct((block, columns), BF16), grant=12 << 20)(
        mixed, gate_two, halo, conv_taps[1]
    )
    return finish(gated, out_weight)


def product_kernel(shifts, weight_ref, before_ref, *refs):
    out_ref = refs[-1]
    peers = weight_ref.shape[0]
    me = lax.axis_index("col")
    half = out_ref.shape[0] // 2
    for part in range(2):
        place = slice(part * half, (part + 1) * half)
        total = None if before_ref is None else before_ref[place, :]
        for shift, ref in zip(shifts, refs):
            term = dot(ref[place, :], weight_ref[lax.rem(me + (peers - shift), peers)])
            total = term if total is None else total + term
        out_ref[place, :] = total.astype(out_ref.dtype)


def first_product(shifts, weight_ref, *refs):
    product_kernel(shifts, weight_ref, None, *refs)


def finish(gated, out_weight):
    peers = lax.axis_size("col")
    columns = gated.shape[1]

    def shifted(block, shift):
        return lax.ppermute(block, "col", [(k, (k + shift) % peers) for k in range(peers)])

    blocks = {0: gated}
    for shift in (2, peers - 2, 1, peers - 1):
        blocks[shift] = shifted(gated, shift)
    blocks[4] = shifted(blocks[2], 2)
    blocks[3] = shifted(blocks[2], 1)
    blocks[peers - 3] = shifted(blocks[peers - 2], peers - 1)
    weight = out_weight.reshape(peers, columns, -1)
    near = (0, 2, peers - 2, 1, peers - 1)
    far = (4, 3, peers - 3)
    shape = (gated.shape[0], weight.shape[2])
    total = call(
        functools.partial(first_product, near),
        jax.ShapeDtypeStruct(shape, F32),
        flops=2_000_000_000,
        grant=12 << 20,
    )(weight, *(blocks[shift] for shift in near))
    return call(
        functools.partial(product_kernel, far), jax.ShapeDtypeStruct(shape, BF16), flops=1_000_000_000, grant=12 << 20
    )(weight, total, *(blocks[shift] for shift in far))


def solution(mesh):
    spread_rows = ("grp", "row")
    in_specs = (
        P(spread_rows, "col"),
        P(spread_rows, "col"),
        P(spread_rows, "col"),
        P(None, None, "col"),
        P(),
        P(),
        P(),
        P(),
        P(),
        P(None, None, None, "col"),
        P(None, None, "col"),
        P(None, "col"),
        P(None, "col"),
    )
    return jax.shard_map(
        per_device, mesh=mesh, in_specs=in_specs, out_specs=P(spread_rows, "col"), check_vma=False
    )
```

```python
import functools
import math

import jax
import jax.numpy as jnp
import numpy as np
from jax import lax
from jax.experimental import pallas as pl
from jax.experimental.pallas import tpu as pltpu
from jax.sharding import PartitionSpec as P

ENERGY_FLOOR = 1.0
UNROLL = 8
F32 = jnp.float32
BF16 = jnp.bfloat16


def halves(value):
    high = value.astype(BF16)
    return high, (value - high.astype(F32)).astype(BF16)


def thirds(value):
    high = value.astype(BF16)
    rest = value - high.astype(F32)
    middle = rest.astype(BF16)
    return high, middle, (rest - middle.astype(F32)).astype(BF16)


def dot(left, right):
    return jnp.dot(left, right, preferred_element_type=F32)


def dot_wide(left_high, left_low, right_high, right_low):
    return dot(
        jnp.concatenate([left_high, left_low, left_high], 1),
        jnp.concatenate([right_high, right_high, right_low], 0),
    )


def cos_turns(turns):
    near = turns - jnp.round(turns)
    quarter = jnp.abs(near) - 0.25
    square = quarter * quarter
    total = jnp.full_like(square, SINE[-1])
    for factor in SINE[-2::-1]:
        total = total * square + factor
    return total * quarter


def fit_sine():
    nodes = 0.25 * np.cos(np.pi * (np.arange(64) + 0.5) / 128)
    powers = np.stack([nodes ** (2 * i + 1) for i in range(4)], 1)
    return [float(v) for v in np.linalg.lstsq(powers, -np.sin(2 * np.pi * nodes), rcond=None)[0]]


SINE = fit_sine()


def split_constant(table):
    high = table.astype(np.float32).astype(jnp.bfloat16)
    return np.stack([high, (table - high.astype(np.float64)).astype(np.float32).astype(jnp.bfloat16)])


@functools.lru_cache
def tables(rows, chan, block):
    waves = 2 * rows
    half = np.arange(rows + 1)
    phase = 2 * np.pi * (half[:, None] * np.arange(rows)[None] % waves) / waves
    weight = np.where((half == 0) | (half == rows), 1.0, 2.0)[:, None] / (waves * block)
    eye = np.eye(chan)
    into = np.concatenate([np.kron(np.cos(phase), eye), np.kron(-np.sin(phase[1:-1]), eye)])
    back = np.concatenate(
        [np.kron(weight * np.cos(phase), eye), np.kron(-(weight * np.sin(phase))[1:-1], eye)]
    ).T
    inner = 2 * np.pi * (np.arange(block)[:, None] * np.arange(block)[None] % block) / block
    pair = np.concatenate([np.cos(inner), np.sin(inner)], 0)
    turn = 2 * np.pi * half[:, None] * np.arange(block)[None] / (waves * block)
    twiddle = np.stack([np.cos(turn), np.sin(turn)]).astype(np.float32)
    return split_constant(into), split_constant(back), split_constant(pair), twiddle


def spread(twiddle_ref, part, chan):
    value = twiddle_ref[part]
    return jnp.broadcast_to(value[:, None, :], (value.shape[0], chan, value.shape[1])).reshape(-1, value.shape[1])


def first_stage(field, into_ref, chan):
    edge = field.shape[0] + chan
    high, low = halves(field)
    part_re = dot_wide(into_ref[0, :edge], into_ref[1, :edge], high, low)
    part_im = dot_wide(into_ref[0, edge:], into_ref[1, edge:], high, low)
    zero = jnp.zeros((chan, field.shape[1]), F32)
    return part_re, jnp.concatenate([zero, part_im, zero], 0)


def pair_product(first, second, pair_ref):
    first_high, first_low = halves(first)
    second_high, second_low = halves(second)
    return dot_wide(
        jnp.concatenate([first_high, second_high], 1),
        jnp.concatenate([first_low, second_low], 1),
        pair_ref[0],
        pair_ref[1],
    )


def forward(field, into_ref, pair_ref, cos_part, sin_part, chan):
    part_re, part_im = first_stage(field, into_ref, chan)
    turned_re = part_re * cos_part + part_im * sin_part
    turned_im = part_im * cos_part - part_re * sin_part
    return pair_product(turned_re, turned_im, pair_ref), pair_product(turned_im, -turned_re, pair_ref)


def backward(part_re, part_im, back_ref, pair_ref, cos_part, sin_part, chan):
    edge = part_re.shape[0]
    wave_re = pair_product(part_re, -part_im, pair_ref)
    wave_im = pair_product(part_im, part_re, pair_ref)
    turned_re = wave_re * cos_part - wave_im * sin_part
    turned_im = wave_re * sin_part + wave_im * cos_part
    high, low = halves(jnp.concatenate([turned_re, turned_im[chan : edge - chan]], 0))
    middle = back_ref.shape[1] // 2
    return jnp.concatenate(
        [
            dot_wide(back_ref[0, :middle], back_ref[1, :middle], high, low),
            dot_wide(back_ref[0, middle:], back_ref[1, middle:], high, low),
        ],
        0,
    )


def filter_kernel(
    rows, chan, embed_ref, first_bias_ref, freq_ref, inner_ref, second_bias_ref, weight_ref, decay_ref, conv_taps_ref,
    skip_ref, band_ref, into_ref, pair_ref, twiddle_ref, spec_re_ref, spec_im_ref, param_ref,
    first_table, second_table, taps_ref, energy_ref, near_ref, far_ref, embed, first_w, second_w, last_w,
    into, pair, arrivals,
):
    fetches = [
        pltpu.make_async_copy(source, target, arrivals.at[k])
        for k, (source, target) in enumerate(((into_ref, into), (pair_ref, pair)))
    ]
    for fetch in fetches:
        fetch.start()
    block = taps_ref.shape[2]
    hidden = freq_ref.shape[1]
    seq_len = rows * block
    orders = skip_ref.shape[0]
    parts = 2 * orders * chan
    width = embed.shape[0]
    columns = skip_ref.shape[1]
    freq = freq_ref[...] * (0.5 / math.pi)
    second_bias = second_bias_ref[...] * freq - 0.25
    count = embed_ref.shape[0]
    embed[...] = jnp.zeros_like(embed)
    embed[:count, :] = embed_ref[...] * freq
    embed[count : count + 1, :] = first_bias_ref[...] * freq - 0.25
    w_one, w_two = halves(embed[...])
    first_w[...] = jnp.concatenate([w_one, w_one, w_two, jnp.zeros_like(w_two)], 0)
    v_one, v_two = halves(inner_ref[...] * freq)
    second_w[:, :hidden] = jnp.concatenate([v_one, v_one], 0)
    second_w[:, hidden:] = jnp.concatenate([v_two, v_two], 0)
    place = lax.broadcasted_iota(jnp.int32, (chan, columns), 1) - lax.axis_index("row") * chan
    chosen = (place == lax.broadcasted_iota(jnp.int32, (chan, columns), 0)).astype(F32).astype(BF16)

    def choose(table):
        return lax.dot_general(chosen, table, (((1,), (1,)), ((), ())), preferred_element_type=F32)

    def choose_exactly(table):
        return sum(choose(part) for part in thirds(table))

    for k in range(2 * orders):
        u_one, u_two = (
            choose(part).astype(BF16) for part in halves(weight_ref[k // 2, k % 2])
        )
        last_w[k * chan : (k + 1) * chan, :] = jnp.concatenate([u_one, u_one], 1)
        last_w[parts + k * chan : parts + (k + 1) * chan, :] = jnp.concatenate([u_two, jnp.zeros_like(u_two)], 1)
    decay = []
    for order in range(orders):
        here = choose_exactly(decay_ref[order])
        decay += [here[:, 0:1], here[:, 1:2]]
    decay = jnp.concatenate(decay, 0)
    for k in range(conv_taps_ref.shape[0]):
        param_ref[k, :, 0:3] = choose(conv_taps_ref[k])
    param_ref[conv_taps_ref.shape[0], :, 0:orders] = choose_exactly(skip_ref[...])
    band = band_ref[0:1]
    shift = band_ref[1:2]
    line = band_ref[2:3]
    lag = lax.broadcasted_iota(jnp.int32, (block, 2 * width), 0).astype(F32)
    turns = lag * band * (1.0 / seq_len)
    first_table[...] = jnp.where(line > 0, 1.0, cos_turns(turns + shift))
    second_table[...] = jnp.where(line > 0, lag * (1.0 / seq_len), cos_turns(turns + (shift + 0.25)))
    start = lax.broadcasted_iota(jnp.int32, (rows, 2 * width), 0).astype(F32)
    turns = start * band * (1.0 / rows)
    near_ref[...] = jnp.where(line > 0, start * (1.0 / rows), cos_turns(turns))
    far_ref[...] = jnp.where(line > 0, 1.0, cos_turns(turns - 0.25))
    energy_ref[...] = jnp.zeros_like(energy_ref)
    lanes = lax.broadcasted_iota(jnp.int32, (1, block), 1)
    left = lax.broadcasted_iota(jnp.int32, (1, 2 * width), 1) < width
    is_back = (lax.broadcasted_iota(jnp.int32, (parts, 1), 0) // chan) % 2 == 1

    def lags(row):
        feature = first_table[...] * near_ref[pl.ds(row, 1), :] + second_table[...] * far_ref[pl.ds(row, 1), :]
        x_one, x_two = halves(feature)
        layer_one = cos_turns(dot(jnp.concatenate([jnp.where(left, x_one, x_two), x_one], 1), first_w[...]))
        y_one, y_two = halves(layer_one)
        both = dot(jnp.concatenate([y_one, y_two], 1), second_w[...])
        layer_two = cos_turns(both[:, :hidden] + both[:, hidden:] + second_bias)
        z_one, z_two = halves(layer_two)
        both = lax.dot_general(
            last_w[...], jnp.concatenate([z_one, z_two], 1), (((1,), (1,)), ((), ())), preferred_element_type=F32
        )
        raw = both[:parts] + both[parts:]
        at = lanes + row * block
        taps = raw * jnp.exp(decay * (at.astype(F32) * (-1.0 / seq_len)))
        return jnp.where(is_back & (at == 0), 0.0, taps)

    @pl.loop(0, rows // UNROLL)
    def _(step):
        found = [lags(UNROLL * step + k) for k in range(UNROLL)]
        energy_ref[...] += sum(taps * taps for taps in found)
        for k in range(UNROLL):
            place = pl.multiple_of((UNROLL * step + k) * chan, chan)
            for order in range(parts // (2 * chan)):
                base = order * 2 * chan
                ahead = found[k][base : base + chan]
                behind = found[k][base + chan : base + 2 * chan]
                taps_ref[2 * order, pl.ds(place, chan), :] = ahead + behind
                taps_ref[2 * order + 1, pl.ds(place, chan), :] = ahead - behind

    for fetch in fetches:
        fetch.wait()
    total = jnp.sum(energy_ref[...], axis=1, keepdims=True)
    cos_part, sin_part = spread(twiddle_ref, 0, chan), spread(twiddle_ref, 1, chan)
    for order in range(parts // (2 * chan)):
        base = order * 2 * chan
        scale = lax.rsqrt(total[base : base + chan] + total[base + chan : base + 2 * chan] + ENERGY_FLOOR)
        scale = jnp.broadcast_to(scale[None], (rows + 1, chan, block)).reshape(-1, block)
        even_re, even_im = first_stage(taps_ref[2 * order], into, chan)
        odd_re, odd_im = first_stage(taps_ref[2 * order + 1], into, chan)
        spec_re_ref[order] = scale * pair_product(
            even_re * cos_part + even_im * sin_part, even_im * cos_part - even_re * sin_part, pair
        )
        spec_im_ref[order] = scale * pair_product(
            odd_im * cos_part - odd_re * sin_part, -(odd_re * cos_part + odd_im * sin_part), pair
        )


def short(signal, taps, rows, chan):
    block = signal.shape[1]
    lanes = lax.broadcasted_iota(jnp.int32, signal.shape, 1)
    line = lax.broadcasted_iota(jnp.int32, signal.shape, 0)
    size = signal.shape[0]
    before = pltpu.roll(signal, 1, 1)
    crossed = jnp.where(line < chan, 0.0, pltpu.roll(before, chan, 0))
    before = jnp.where(lanes == 0, crossed, before)
    after = pltpu.roll(signal, block - 1, 1)
    crossed = jnp.where(line >= size - chan, 0.0, pltpu.roll(after, size - chan, 0))
    after = jnp.where(lanes == block - 1, crossed, after)

    def tap(k):
        column = taps[:, k : k + 1]
        return jnp.broadcast_to(column[None], (rows, chan, block)).reshape(size, block)

    return before * tap(0) + signal * tap(1) + after * tap(2)


def conv_kernel(
    rows, chan, orders, arrived_ref, param_ref, spec_re_ref, spec_im_ref, into_ref, back_ref, pair_ref,
    twiddle_ref, out_ref,
):
    block = arrived_ref.shape[2]
    size = rows * chan

    def signal(k):
        return arrived_ref[:, k * chan : (k + 1) * chan, :].astype(F32).reshape(size, block)

    cos_part, sin_part = spread(twiddle_ref, 0, chan), spread(twiddle_ref, 1, chan)
    current = short(signal(0), param_ref[orders], rows, chan)
    for order in range(orders):
        data_re, data_im = forward(current, into_ref, pair_ref, cos_part, sin_part, chan)
        spec_re, spec_im = spec_re_ref[order], spec_im_ref[order]
        long_part = backward(
            data_re * spec_re - data_im * spec_im,
            data_re * spec_im + data_im * spec_re,
            back_ref, pair_ref, cos_part, sin_part, chan,
        )
        column = param_ref[orders + 1, :, order : order + 1]
        skip = jnp.broadcast_to(column[None], (rows, chan, block)).reshape(size, block)
        current = long_part + skip * current
        if order < orders - 1:
            current = current * short(signal(order + 1), param_ref[order], rows, chan)
    out_ref[...] = current.astype(BF16).reshape(rows, chan, block)


def turn_kernel(first_ref, second_ref, out_ref, first, second, first_out, second_out, arrivals, departures):
    chan = out_ref.shape[1] // 2
    moves = []
    for k, (ref, held, turned) in enumerate(((first_ref, first, first_out), (second_ref, second, second_out))):
        fetch = pltpu.make_async_copy(ref, held, arrivals.at[k])
        fetch.start()
        leave = pltpu.make_async_copy(turned, out_ref.at[:, pl.ds(k * chan, chan), :], departures.at[k])
        moves.append((fetch, held, turned, leave))
    for fetch, held, turned, leave in moves:
        fetch.wait()
        turned[...] = jnp.transpose(held[...].astype(F32)).astype(BF16).reshape(turned.shape)
        leave.start()
    for _, _, _, leave in moves:
        leave.wait()


def gate_kernel(mixed_ref, gate_ref, halo_ref, taps_ref, out_ref):
    gate = gate_ref[...].astype(F32)
    block = gate.shape[0]
    line = lax.broadcasted_iota(jnp.int32, gate.shape, 0)
    halo = halo_ref[...].astype(F32)
    taps = taps_ref[...].astype(F32)
    before = jnp.where(line == 0, halo[0:1], pltpu.roll(gate, 1, 0))
    after = jnp.where(line == block - 1, halo[1:2], pltpu.roll(gate, block - 1, 0))
    factor = before * taps[0:1] + gate * taps[1:2] + after * taps[2:3]
    out_ref[...] = (jnp.transpose(mixed_ref[...].astype(F32)) * factor).astype(BF16)


def call(kernel, out_shape, scratch=(), flops=0, grant=None, placed=None, result=None):
    specs = {} if placed is None else {"in_specs": [pl.BlockSpec(memory_space=space) for space in placed]}
    if result is not None:
        specs["out_specs"] = pl.BlockSpec(memory_space=result)
    return pl.pallas_call(
        kernel,
        out_shape=out_shape,
        **specs,
        scratch_shapes=scratch,
        cost_estimate=pl.CostEstimate(flops=flops, bytes_accessed=0, transcendentals=0),
        compiler_params=pltpu.CompilerParams(vmem_limit_bytes=grant),
    )


def per_device(
    gate_one, gate_two, values, conv_taps, embed_weight, embed_bias, sine_freq, inner_weight, inner_bias,
    filter_weight, decay_rate, skip_gain, out_weight,
):
    rows = lax.axis_size("row")
    block, columns = gate_one.shape
    orders = skip_gain.shape[0]
    chan = columns // rows
    hidden = sine_freq.shape[0]
    features = embed_weight.shape[0]
    bands = (features - 1) // 2
    into, back, pair, twiddle = tables(rows, chan, block)

    vmem, anywhere = pltpu.VMEM, pl.ANY
    turned = call(
        turn_kernel,
        jax.ShapeDtypeStruct((rows, 2 * chan, block), BF16),
        [pltpu.VMEM((block, columns), BF16)] * 2
        + [pltpu.VMEM((rows, chan, block), BF16)] * 2
        + [pltpu.SemaphoreType.DMA((2,))] * 2,
        placed=[anywhere] * 2,
        result=anywhere,
    )(values, gate_one)
    arrived = lax.all_to_all(turned, "row", 0, 0, tiled=True)

    down = [(k, k + 1) for k in range(rows - 1)]
    up = [(k + 1, k) for k in range(rows - 1)]
    halo = [lax.ppermute(gate_two[-1:], "row", down), lax.ppermute(gate_two[:1], "row", up)]
    halo = jnp.concatenate(halo, 0)

    width = 64
    steps = np.linspace(0.0001, bands - 1, bands).astype(np.float32)
    band = np.zeros((3, width), np.float32)
    band[0, 1:features] = np.concatenate([steps, steps])
    band[1, 1 + bands : features] = 0.25
    band[2, 0] = 1
    band[:, features:] = 0
    band = np.concatenate([band, band], 1)

    edge = (rows + 1) * chan
    parts = 2 * orders * chan
    spec_shape = jax.ShapeDtypeStruct((orders, edge, block), F32)
    spec_re, spec_im, param = call(
        functools.partial(filter_kernel, rows, chan),
        (spec_shape, spec_shape, jax.ShapeDtypeStruct((conv_taps.shape[0] + 1, chan, 4), F32)),
        (
            pltpu.VMEM((block, 2 * width), F32),
            pltpu.VMEM((block, 2 * width), F32),
            pltpu.VMEM((parts // chan, rows * chan, block), F32),
            pltpu.VMEM((parts, block), F32),
            pltpu.VMEM((rows, 2 * width), F32),
            pltpu.VMEM((rows, 2 * width), F32),
            pltpu.VMEM((width, hidden), F32),
            pltpu.VMEM((4 * width, hidden), BF16),
            pltpu.VMEM((2 * hidden, 2 * hidden), BF16),
            pltpu.VMEM((2 * parts, 2 * hidden), BF16),
            pltpu.VMEM(into.shape, BF16),
            pltpu.VMEM(pair.shape, BF16),
            pltpu.SemaphoreType.DMA((2,)),
        ),
        flops=12_000_000_000,
        placed=[vmem] * 10 + [anywhere] * 2 + [vmem],
    )(
        embed_weight, embed_bias[None], sine_freq[None], inner_weight, inner_bias[None],
        jnp.transpose(filter_weight, (1, 2, 0, 3)), decay_rate, conv_taps, skip_gain, band, into, pair, twiddle,
    )
    mixed = call(
        functools.partial(conv_kernel, rows, chan, orders),
        jax.ShapeDtypeStruct((rows, chan, block), BF16),
        flops=5_000_000_000,
        grant=53 << 20,
    )(arrived, param, spec_re, spec_im, into, back, pair, twiddle)
    mixed = lax.all_to_all(mixed, "row", 0, 0, tiled=True).reshape(columns, block)
    gated = call(gate_kernel, jax.ShapeDtypeStruct((block, columns), BF16), grant=12 << 20)(
        mixed, gate_two, halo, conv_taps[1]
    )
    return finish(gated, out_weight)


def product_kernel(shifts, weight_ref, before_ref, *refs):
    out_ref = refs[-1]
    peers = weight_ref.shape[0]
    me = lax.axis_index("col")
    half = out_ref.shape[0] // 2
    for part in range(2):
        place = slice(part * half, (part + 1) * half)
        total = None if before_ref is None else before_ref[place, :]
        for shift, ref in zip(shifts, refs):
            term = dot(ref[place, :], weight_ref[lax.rem(me + (peers - shift), peers)])
            total = term if total is None else total + term
        out_ref[place, :] = total.astype(out_ref.dtype)


def first_product(shifts, weight_ref, *refs):
    product_kernel(shifts, weight_ref, None, *refs)


def finish(gated, out_weight):
    peers = lax.axis_size("col")
    columns = gated.shape[1]

    def shifted(block, shift):
        return lax.ppermute(block, "col", [(k, (k + shift) % peers) for k in range(peers)])

    blocks = {0: gated}
    for shift in (2, peers - 2, 1, peers - 1):
        blocks[shift] = shifted(gated, shift)
    blocks[4] = shifted(blocks[2], 2)
    blocks[3] = shifted(blocks[2], 1)
    blocks[peers - 3] = shifted(blocks[peers - 2], peers - 1)
    weight = out_weight.reshape(peers, columns, -1)
    near = (0, 2, peers - 2, 1, peers - 1)
    far = (4, 3, peers - 3)
    shape = (gated.shape[0], weight.shape[2])
    total = call(
        functools.partial(first_product, near),
        jax.ShapeDtypeStruct(shape, F32),
        flops=2_000_000_000,
        grant=12 << 20,
    )(weight, *(blocks[shift] for shift in near))
    return call(
        functools.partial(product_kernel, far), jax.ShapeDtypeStruct(shape, BF16), flops=1_000_000_000, grant=12 << 20
    )(weight, total, *(blocks[shift] for shift in far))


def solution(mesh):
    spread_rows = ("grp", "row")
    in_specs = (
        P(spread_rows, "col"),
        P(spread_rows, "col"),
        P(spread_rows, "col"),
        P(None, None, "col"),
        P(),
        P(),
        P(),
        P(),
        P(),
        P(None, None, None, "col"),
        P(None, None, "col"),
        P(None, "col"),
        P(None, "col"),
    )
    return jax.shard_map(
        per_device, mesh=mesh, in_specs=in_specs, out_specs=P(spread_rows, "col"), check_vma=False
    )
```
